256 devices in a mesh: kv: 64 (over z, x, core), tp: 4 (over y).
Axes of the slice: x: 4, y: 4, z: 8, core: 2. Of those that a mesh axis runs over, the one named last changes fastest.
Arguments:
- hidden: bfloat16 [1024, 4, 2048], P(None, None, 'kv'), may hold values from -18 to 18
- norm_gain: float32 [2048], replicated, may hold values from 0.1 to 1.9
- w_query: bfloat16 [2048, 1024], P(None, 'tp'), may hold values from -0.125 to 0.125
- w_forget: bfloat16 [2048, 1024], P(None, 'tp'), may hold values from -0.125 to 0.125
- w_input: bfloat16 [2048, 1024], P(None, 'tp'), may hold values from -0.125 to 0.125
- w_outgate: bfloat16 [2048, 1024], P(None, 'tp'), may hold values from -0.125 to 0.125
- w_out: bfloat16 [1024, 2048], replicated, may hold values from -0.1875 to 0.1875
- floor: float32 [1024], P('tp'), may hold values from 0 to 0.95
- head_gain: float32 [128], replicated, may hold values from 0.1 to 1.9
- base_state: float32 [1024, 8, 128, 128], P('kv', 'tp'), may hold values from -4 to 4
- prev_forget: bfloat16 [1024, 4, 1024], P('kv', None, 'tp'), may hold values from -6 to 6
- prev_input: bfloat16 [1024, 4, 1024], P('kv', None, 'tp'), may hold values from -6 to 6
- accepted: int32 [1024], P('kv'), may hold values from 0 to 4
Outputs:
- mixed: bfloat16 [1024, 4, 2048], P(None, None, 'kv')
- taken_state: float32 [1024, 8, 128, 128], P('kv', 'tp')
The draws below stay inside these ranges and needn't reach their ends.
All inputs are finite; a program needn't handle non-finite values.
Results may differ from the reference program's by a relative error of at most 0.014.
Values may be sent and summed in bfloat16 or wider, within the bound.
A program may use at most 64 MiB of HBM per device.

```python
import jax
import jax.numpy as jnp
from jax import lax

D = 2048
HEADS = 8
HEAD_DIM = 128
PROPS = 4
SEQ_DEV = 16
WIDTH = 1024
SEQS = 1024
N_KV = 64


def draw_hidden(key, part):
    columns = jnp.arange(D, dtype=jnp.float32) / D
    base = jnp.clip(jax.random.normal(key, (SEQ_DEV * N_KV, PROPS, D), jnp.float32), -6.0, 6.0)
    return (base * 3.0 ** columns).astype(jnp.bfloat16)


def touch_ends(entries, stream_key, smallest, top_value):
    longest = entries.shape.index(max(entries.shape))
    spots = []
    for shift in (0, 1):
        where = [jax.random.randint(jax.random.fold_in(stream_key, axis), (), 0, length) for axis, length in enumerate(entries.shape)]
        where[longest] = (where[longest] + shift) % entries.shape[longest]
        spots.append(tuple(where))
    return entries.at[spots[0]].set(smallest).at[spots[1]].set(top_value)


def levels(stream_key, shape, pieces, least, high):
    def one(dim, parts):
        steps = jax.random.uniform(jax.random.fold_in(jax.random.fold_in(stream_key, 6), dim), (parts,), jnp.float32, least / len(pieces), high / len(pieces))
        return jnp.repeat(jnp.exp(steps), shape[dim] // parts).reshape((-1,) + (1,) * (len(shape) - dim - 1))

    loudness = one(*pieces[0])
    for cut in pieces[1:]:
        loudness = loudness * one(*cut)
    return loudness


def centred(key, extent, width, reach, cuts=(), held_as=jnp.bfloat16):
    loudness = levels(key, extent, cuts, -0.22, 0.18) if cuts else 1.0
    values = jax.random.normal(key, extent, jnp.float32) * width * loudness
    return jnp.minimum(jnp.maximum(values, -reach), reach).astype(held_as)


def setup_inputs(seed: int = 0) -> dict:
    splits = jax.random.split(jax.random.key(seed), 14)
    hidden = draw_hidden(jax.random.fold_in(splits[13], 71), 0)
    norm_gain = jnp.clip(1.0 + 0.18 * jax.random.normal(splits[1], (D,), jnp.float32), 0.1, 1.9)
    w_query = centred(splits[2], (D, WIDTH), D ** -0.5, 0.125, ((1, 4),))
    w_forget = centred(splits[3], (D, WIDTH), D ** -0.5, 0.125, ((1, 4),))
    w_input = centred(splits[4], (D, WIDTH), D ** -0.5, 0.125, ((1, 4),))
    w_outgate = centred(splits[5], (D, WIDTH), D ** -0.5, 0.125, ((1, 4),))
    w_out = centred(splits[6], (WIDTH, D), WIDTH ** -0.5, 0.1875)
    floor = jnp.clip(0.95 * jax.random.uniform(splits[7], (WIDTH,), jnp.float32) ** levels(splits[7], (WIDTH,), ((0, 4),), -0.2, 0.2), 0.0, 0.95)
    head_gain = jnp.clip(1.0 + 0.18 * jax.random.normal(splits[8], (HEAD_DIM,), jnp.float32), 0.1, 1.9)
    base_state = centred(splits[9], (SEQS, HEADS, HEAD_DIM, HEAD_DIM), 0.3, 4.0, ((0, 64), (1, 4)), jnp.float32)
    prev_forget = centred(splits[10], (SEQS, PROPS, WIDTH), 1.5, 6.0, ((0, 64), (2, 4)))
    prev_input = centred(splits[11], (SEQS, PROPS, WIDTH), 1.0, 6.0, ((0, 64), (2, 4)))
    accepted = touch_ends(jax.random.randint(splits[12], (SEQS,), 0, PROPS + 1), jax.random.fold_in(splits[12], 1), 0, PROPS).astype(jnp.int32)
    return {"hidden": hidden, "norm_gain": norm_gain, "w_query": w_query, "w_forget": w_forget, "w_input": w_input, "w_outgate": w_outgate, "w_out": w_out, "floor": floor, "head_gain": head_gain, "base_state": base_state, "prev_forget": prev_forget, "prev_input": prev_input, "accepted": accepted}


def reference(hidden, norm_gain, w_query, w_forget, w_input, w_outgate, w_out, floor, head_gain, base_state, prev_forget, prev_input, accepted):
    values_in = hidden.astype(jnp.float32)
    squares = lax.optimization_barrier(jnp.sum(values_in * values_in, axis=2))
    normed = (values_in * lax.rsqrt(squares / D + 1e-06)[..., None] * norm_gain).astype(jnp.bfloat16)
    query_pre = jnp.dot(normed, w_query, preferred_element_type=jnp.float32).astype(jnp.bfloat16)
    forget_pre = jnp.dot(normed, w_forget, preferred_element_type=jnp.float32).astype(jnp.bfloat16)
    input_pre = jnp.dot(normed, w_input, preferred_element_type=jnp.float32).astype(jnp.bfloat16)
    gate_pre = jnp.dot(normed, w_outgate, preferred_element_type=jnp.float32).astype(jnp.bfloat16)
    seqs = hidden.shape[0]
    shape = (seqs, PROPS, HEADS, HEAD_DIM)
    query = jax.nn.silu(query_pre.astype(jnp.float32)).reshape(shape)
    forget = (floor + (1.0 - floor) * jax.nn.sigmoid(forget_pre.astype(jnp.float32))).reshape(shape)
    value = input_pre.astype(jnp.float32).reshape(shape)
    prev_f = (floor + (1.0 - floor) * jax.nn.sigmoid(prev_forget.astype(jnp.float32))).reshape(shape)
    prev_v = prev_input.astype(jnp.float32).reshape(shape)
    state = base_state
    for step in range(PROPS):
        live = (step < accepted)[:, None, None, None]
        moved = prev_f[:, step][..., None] * state + (1.0 - prev_f[:, step])[..., None] * prev_v[:, step][:, :, None, :]
        state = jnp.where(live, moved, state)
    taken_state = state
    outputs = []
    for step in range(PROPS):
        state = forget[:, step][..., None] * state + (1.0 - forget[:, step])[..., None] * value[:, step][:, :, None, :]
        outputs.append(jnp.einsum('bhk,bhkv->bhv', query[:, step], state, precision=lax.Precision.HIGHEST))
    result = jnp.stack(outputs, axis=1)
    scaled = result * lax.rsqrt(lax.optimization_barrier(jnp.mean(result * result, axis=-1, keepdims=True)) + 1e-05) * head_gain
    gated = scaled * jax.nn.silu(gate_pre.astype(jnp.float32)).reshape(shape)
    mixed_heads = gated.reshape(seqs, PROPS, HEADS * HEAD_DIM).astype(jnp.bfloat16)
    mixed = jnp.dot(mixed_heads, w_out, preferred_element_type=jnp.float32).astype(jnp.bfloat16)
    return (mixed, taken_state)
```

```python
import functools

import jax
import jax.numpy as jnp
from jax import lax
from jax.experimental import pallas as pl
from jax.experimental.pallas import tpu as pltpu
from jax.sharding import PartitionSpec as P

D = 2048
HD = 128
PROPS = 4
NKV = 64
NTP = 4
SEQ = 16
ROWS = SEQ * PROPS
F = D // NKV
MESH = pl.DeviceIdType.MESH
FAR_FIRST = (4, 3, 5, 2, 6, 1, 7, 0)
NEAR_FIRST = (0, 1, 7, 2, 6, 3, 5, 4)


def swap_blocks(parts):
    lane = lax.broadcasted_iota(jnp.int32, parts[0].shape, parts[0].ndim - 1)
    axis = parts[0].ndim - 1
    low = lane < 64
    even = (lane // 32) % 2 == 0
    a0, a1, a2, a3 = parts
    c0 = jnp.where(low, a0, pltpu.roll(a2, 64, axis))
    c2 = jnp.where(low, pltpu.roll(a0, 64, axis), a2)
    c1 = jnp.where(low, a1, pltpu.roll(a3, 64, axis))
    c3 = jnp.where(low, pltpu.roll(a1, 64, axis), a3)
    b0 = jnp.where(even, c0, pltpu.roll(c1, 32, axis))
    b1 = jnp.where(even, pltpu.roll(c0, 96, axis), c1)
    b2 = jnp.where(even, c2, pltpu.roll(c3, 32, axis))
    b3 = jnp.where(even, pltpu.roll(c2, 96, axis), c3)
    return b0, b1, b2, b3


def sigmoid(x):
    return jax.nn.sigmoid(x)


def kernel(
    x_hbm, gain_hbm, wq_hbm, wf_hbm, wi_hbm, wg_hbm, wo_hbm, floor_hbm, hgain_hbm,
    base_hbm, pf_hbm, pv_hbm, acc_hbm,
    mixed_ref, taken_ref,
    x_v, gain_v, w_v, wo_v, floor_v, hgain_v, base_v, pf_v, pv_v, acc_v,
    s0_v, tx1, rx1, pre_v, a_v, o_v, mh_v, tx2, rx2,
    lsem, ssem1, rsem1, ssem2, rsem2, ssem3, rsem3,
):
    kv = lax.axis_index("kv")
    tp = lax.axis_index("tp")
    z = kv // 8
    xc = kv % 8

    locals_ = [
        pltpu.make_async_copy(x_hbm, x_v, lsem.at[0]),
        pltpu.make_async_copy(pf_hbm, pf_v, lsem.at[1]),
        pltpu.make_async_copy(pv_hbm, pv_v, lsem.at[2]),
        pltpu.make_async_copy(acc_hbm, acc_v, lsem.at[3]),
        pltpu.make_async_copy(floor_hbm, floor_v, lsem.at[4]),
        pltpu.make_async_copy(base_hbm, base_v, lsem.at[5]),
        pltpu.make_async_copy(gain_hbm, gain_v, lsem.at[6]),
        pltpu.make_async_copy(wq_hbm, w_v.at[0], lsem.at[7]),
        pltpu.make_async_copy(wf_hbm, w_v.at[1], lsem.at[8]),
        pltpu.make_async_copy(wi_hbm, w_v.at[2], lsem.at[9]),
        pltpu.make_async_copy(wg_hbm, w_v.at[3], lsem.at[10]),
        pltpu.make_async_copy(hgain_hbm, hgain_v, lsem.at[11]),
        pltpu.make_async_copy(wo_hbm, wo_v, lsem.at[12]),
    ]
    for copy in locals_:
        copy.start()

    barrier = pltpu.get_barrier_semaphore()

    def greet(k, c):
        pl.semaphore_signal(barrier, inc=1, device_id={"kv": (kv + k) % NKV}, device_id_type=MESH)
        return c

    lax.fori_loop(1, NKV, greet, 0)
    for k in range(1, NTP):
        pl.semaphore_signal(barrier, inc=1, device_id={"tp": (tp + k) % NTP}, device_id_type=MESH)

    locals_[0].wait()
    for b in range(8):
        block = x_v[:, :, 128 * b : 128 * (b + 1)].reshape(128, 128)
        tx1[8 * b : 8 * (b + 1)] = jnp.transpose(block).reshape(8, SEQ, 128)

    pl.semaphore_wait(barrier, NKV - 1 + NTP - 1)

    def send1(zd, xd):
        d = zd * 8 + xd
        pltpu.make_async_remote_copy(
            src_ref=tx1.at[d], dst_ref=rx1.at[kv], send_sem=ssem1, recv_sem=rsem1.at[z],
            device_id={"kv": d}, device_id_type=MESH,
        ).start()

    for dist in FAR_FIRST:
        zd = (z + dist) % 8
        lax.fori_loop(1 if dist == 0 else 0, 8, lambda k, c: (send1(zd, (xc + k) % 8), c)[1], 0)
    rx1[kv] = tx1[kv]

    for i in range(1, 6):
        locals_[i].wait()
    fl = floor_v[...]
    row4 = lax.broadcasted_iota(jnp.int32, (PROPS, 2 * HD), 0)
    seq_lane = lax.broadcasted_iota(jnp.int32, (1, SEQ), 1)

    def state_step(s, c):
        count = jnp.sum(jnp.where(seq_lane == s, acc_v[...], 0), axis=1, keepdims=True)
        live = row4 < count
        f = fl + (1.0 - fl) * sigmoid(pf_v[s].astype(jnp.float32))
        k = jnp.where(live, 1.0 - f, 0.0)
        f = jnp.where(live, f, 1.0)
        v = pv_v[s].astype(jnp.float32)
        f0, f1, f2, f3 = (f[j : j + 1] for j in range(4))
        f23 = f2 * f3
        f123 = f1 * f23
        stack = jnp.concatenate(
            [f0 * f123, k[0:1] * f123, k[1:2] * f23, k[2:3] * f3, k[3:4], jnp.zeros((3, 2 * HD), jnp.float32)],
            axis=0,
        )
        for h in range(2):
            cols = jnp.transpose(stack[:, h * HD : (h + 1) * HD])
            new = cols[:, 0:1] * base_v[s, h]
            for j in range(4):
                new = new + cols[:, j + 1 : j + 2] * v[j : j + 1, h * HD : (h + 1) * HD]
            taken_ref[s, h] = new
            s0_v[s, h] = new.astype(jnp.bfloat16)
        return c

    lax.fori_loop(0, SEQ, state_step, 0)

    for i in range(6, 11):
        locals_[i].wait()
    squares = jnp.zeros((SEQ, 128), jnp.float32)
    for n, dist in enumerate(NEAR_FIRST):
        zs = (z + dist) % 8
        count = 7 if dist == 0 else 8
        group = rx1.at[pl.ds(0, count)] if dist == 0 else rx1.at[pl.ds(pl.multiple_of(zs * 8, 8), count)]
        pltpu.make_async_remote_copy(
            src_ref=group, dst_ref=group, send_sem=ssem1, recv_sem=rsem1.at[zs],
            device_id={"kv": kv}, device_id_type=MESH,
        ).wait_recv()
        vals = rx1[pl.ds(pl.multiple_of(zs * 8, 8), 8)].astype(jnp.float32)
        squares = squares + jnp.sum(vals * vals, axis=0)
        tiles = []
        for q in range(2):
            swapped = swap_blocks([vals[4 * q + i] for i in range(4)])
            gain = gain_v[:, pl.ds(pl.multiple_of(zs * 256 + q * 128, 128), 128)]
            tiles.append(jnp.concatenate([(part * gain).astype(jnp.bfloat16) for part in swapped], axis=0))
        lhs = jnp.concatenate(tiles, axis=1)
        for i in range(4):
            w = w_v[i, pl.ds(pl.multiple_of(zs * 256, 256), 256), :]
            prod = jnp.dot(lhs, w, preferred_element_type=jnp.float32)
            if n == 0:
                pre_v[i] = prod
            else:
                pre_v[i] += prod
    lane = lax.broadcasted_iota(jnp.int32, (SEQ, 128), 1)
    scale = jnp.concatenate(
        [
            lax.rsqrt(
                jnp.sum(jnp.where(lane // F == p, squares, 0.0), axis=1, keepdims=True) / D + 1e-06
            )
            for p in range(PROPS)
        ],
        axis=0,
    )

    def pre(i):
        return (pre_v[i] * scale).astype(jnp.bfloat16).astype(jnp.float32)

    q_all = pre(0)
    q_all = q_all * sigmoid(q_all)
    f_all = fl + (1.0 - fl) * sigmoid(pre(1))
    k_all = 1.0 - f_all
    v_all = pre(2)

    def at(arr, t):
        return arr[t * SEQ : (t + 1) * SEQ]

    decay = None
    for t in range(PROPS):
        decay = at(f_all, t) if t == 0 else decay * at(f_all, t)
        for h in range(2):
            a_v[h, t * SEQ : (t + 1) * SEQ, :] = (at(q_all, t) * decay)[:, h * HD : (h + 1) * HD]
    for s in range(SEQ):
        for h in range(2):
            lhs = a_v[h, pl.ds(s, PROPS, stride=SEQ), :].astype(jnp.bfloat16)
            o_v[h, pl.ds(s, PROPS, stride=SEQ), :] = jnp.dot(
                lhs, s0_v[s, h], preferred_element_type=jnp.float32
            )
    locals_[11].wait()
    hg = hgain_v[...]
    gate = pre(3)
    gate = gate * sigmoid(gate)
    for t in range(PROPS):
        weight = at(q_all, t)
        extra = [jnp.zeros((SEQ, HD), jnp.float32) for _ in range(2)]
        for j in range(t, -1, -1):
            term = weight * at(k_all, j)
            for h in range(2):
                c = jnp.sum(term[:, h * HD : (h + 1) * HD], axis=1, keepdims=True)
                extra[h] = extra[h] + c * at(v_all, j)[:, h * HD : (h + 1) * HD]
            weight = weight * at(f_all, j)
        for h in range(2):
            cols = slice(h * HD, (h + 1) * HD)
            o = o_v[h, t * SEQ : (t + 1) * SEQ, :] + extra[h]
            norm = lax.rsqrt(jnp.mean(o * o, axis=1, keepdims=True) + 1e-05)
            mh_v[tp, t * SEQ : (t + 1) * SEQ, cols] = (
                o * norm * hg * at(gate, t)[:, cols]
            ).astype(jnp.bfloat16)

    gathers = []
    for k in range(1, NTP):
        copy = pltpu.make_async_remote_copy(
            src_ref=mh_v.at[tp], dst_ref=mh_v.at[tp], send_sem=ssem2.at[k], recv_sem=rsem2.at[k],
            device_id={"tp": (tp + k) % NTP}, device_id_type=MESH,
        )
        copy.start()
        gathers.append(copy)
    locals_[12].wait()
    for copy in gathers:
        copy.wait()

    for dist in FAR_FIRST:
        zd = (z + dist) % 8
        out = None
        for a in range(NTP):
            w = wo_v[a * 256 : (a + 1) * 256, pl.ds(pl.multiple_of(zd * 256, 256), 256)]
            prod = jnp.dot(mh_v[a], w, preferred_element_type=jnp.float32)
            out = prod if out is None else out + prod
        for q in range(2):
            blocks = swap_blocks([out[p * SEQ : (p + 1) * SEQ, q * 128 : (q + 1) * 128] for p in range(PROPS)])
            for j in range(4):
                tx2[zd * 8 + 4 * q + j] = blocks[j].astype(jnp.bfloat16)

        def send2(k, c):
            d = zd * 8 + (xc + k) % 8
            pltpu.make_async_remote_copy(
                src_ref=tx2.at[d], dst_ref=rx2.at[kv], send_sem=ssem3, recv_sem=rsem3.at[z],
                device_id={"kv": d}, device_id_type=MESH,
            ).start()
            return c

        lax.fori_loop(1 if dist == 0 else 0, 8, send2, 0)
    rx2[kv] = tx2[kv]

    for dist in NEAR_FIRST:
        zs = (z + dist) % 8
        count = 7 if dist == 0 else 8
        group = rx2.at[pl.ds(0, count)] if dist == 0 else rx2.at[pl.ds(pl.multiple_of(zs * 8, 8), count)]
        pltpu.make_async_remote_copy(
            src_ref=group, dst_ref=group, send_sem=ssem3, recv_sem=rsem3.at[zs],
            device_id={"kv": kv}, device_id_type=MESH,
        ).wait_recv()
        block = rx2[pl.ds(pl.multiple_of(zs * 8, 8), 8)].reshape(128, 128)
        mixed_ref[:, :, pl.ds(pl.multiple_of(zs * 128, 128), 128)] = jnp.transpose(block).reshape(
            PROPS, F, 128
        )

    for tx, sem in ((tx1, ssem1), (tx2, ssem3)):
        sent = tx.at[pl.ds(0, NKV - 1)]
        pltpu.make_async_remote_copy(
            src_ref=sent, dst_ref=sent, send_sem=sem, recv_sem=sem,
            device_id={"kv": kv}, device_id_type=MESH,
        ).wait_send()


def shards(hidden, norm_gain, w_query, w_forget, w_input, w_outgate, w_out, floor, head_gain, base_state, prev_forget, prev_input, accepted):
    any_spec = pl.BlockSpec(memory_space=pl.ANY)
    vmem = pl.BlockSpec(memory_space=pltpu.VMEM)
    bf, f32 = jnp.bfloat16, jnp.float32
    mixed, taken = pl.pallas_call(
        kernel,
        name="verify",
        out_shape=(
            jax.ShapeDtypeStruct((PROPS, F, NKV * SEQ), bf),
            jax.ShapeDtypeStruct((SEQ, 2, HD, HD), f32),
        ),
        in_specs=[any_spec] * 13,
        out_specs=(vmem, vmem),
        scratch_shapes=[
            pltpu.VMEM((PROPS, F, NKV * SEQ), bf),
            pltpu.VMEM((1, D), f32),
            pltpu.VMEM((4, D, 256), bf),
            pltpu.VMEM((1024, D), bf),
            pltpu.VMEM((1, 256), f32),
            pltpu.VMEM((1, HD), f32),
            pltpu.VMEM((SEQ, 2, HD, HD), f32),
            pltpu.VMEM((SEQ, PROPS, 256), bf),
            pltpu.VMEM((SEQ, PROPS, 256), bf),
            pltpu.VMEM((1, SEQ), jnp.int32),
            pltpu.VMEM((SEQ, 2, HD, HD), bf),
            pltpu.VMEM((NKV, SEQ, 128), bf),
            pltpu.VMEM((NKV, SEQ, 128), bf),
            pltpu.VMEM((4, ROWS, 256), f32),
            pltpu.VMEM((2, ROWS, HD), f32),
            pltpu.VMEM((2, ROWS, HD), f32),
            pltpu.VMEM((NTP, ROWS, 256), bf),
            pltpu.VMEM((NKV, SEQ, 128), bf),
            pltpu.VMEM((NKV, SEQ, 128), bf),
            pltpu.SemaphoreType.DMA((13,)),
            pltpu.SemaphoreType.DMA,
            pltpu.SemaphoreType.DMA((8,)),
            pltpu.SemaphoreType.DMA((NTP,)),
            pltpu.SemaphoreType.DMA((NTP,)),
            pltpu.SemaphoreType.DMA,
            pltpu.SemaphoreType.DMA((8,)),
        ],
        compiler_params=pltpu.CompilerParams(collective_id=0, has_side_effects=True),
    )(
        jnp.transpose(hidden, (1, 2, 0)),
        norm_gain.reshape(1, -1),
        w_query, w_forget, w_input, w_outgate, w_out,
        floor.reshape(1, -1),
        head_gain.reshape(1, -1),
        base_state, prev_forget, prev_input,
        accepted.reshape(1, -1),
    )
    return jnp.transpose(mixed, (2, 0, 1)), taken


def solution(mesh):
    in_specs = (
        P(None, None, "kv"), P(), P(None, "tp"), P(None, "tp"), P(None, "tp"), P(None, "tp"), P(), P("tp"), P(),
        P("kv", "tp", None, None), P("kv", None, "tp"), P("kv", None, "tp"), P("kv"),
    )
    out_specs = (P(None, None, "kv"), P("kv", "tp", None, None))
    return jax.shard_map(shards, mesh=mesh, in_specs=in_specs, out_specs=out_specs, check_vma=False)
```

```python
import functools

import jax
import jax.numpy as jnp
from jax import lax
from jax.experimental import pallas as pl
from jax.experimental.pallas import tpu as pltpu
from jax.sharding import PartitionSpec as P

D = 2048
HD = 128
PROPS = 4
NKV = 64
NTP = 4
SEQ = 16
ROWS = SEQ * PROPS
F = D // NKV
EARLY = 4
MESH = pl.DeviceIdType.MESH
FAR_FIRST = (3, 5, 2, 6, 1, 7, 0)


def swap_blocks(parts):
    lane = lax.broadcasted_iota(jnp.int32, parts[0].shape, parts[0].ndim - 1)
    axis = parts[0].ndim - 1
    low = lane < 64
    even = (lane // 32) % 2 == 0
    a0, a1, a2, a3 = parts
    c0 = jnp.where(low, a0, pltpu.roll(a2, 64, axis))
    c2 = jnp.where(low, pltpu.roll(a0, 64, axis), a2)
    c1 = jnp.where(low, a1, pltpu.roll(a3, 64, axis))
    c3 = jnp.where(low, pltpu.roll(a1, 64, axis), a3)
    b0 = jnp.where(even, c0, pltpu.roll(c1, 32, axis))
    b1 = jnp.where(even, pltpu.roll(c0, 96, axis), c1)
    b2 = jnp.where(even, c2, pltpu.roll(c3, 32, axis))
    b3 = jnp.where(even, pltpu.roll(c2, 96, axis), c3)
    return b0, b1, b2, b3


def sigmoid(x):
    return jax.nn.sigmoid(x)


def kernel(
    x_hbm, gain_hbm, wq_hbm, wf_hbm, wi_hbm, wg_hbm, wo_hbm, floor_hbm, hgain_hbm,
    base_hbm, pf_hbm, pv_hbm, acc_hbm,
    mixed_ref, taken_ref,
    x_v, gain_v, w_v, wo_v, floor_v, hgain_v, base_v, pf_v, pv_v, acc_v,
    s0_v, tx1, rx1, pre_v, a_v, o_v, mh_v, tx2, rx2,
    acc_o,
    lsem, ssem1, rsem1, ssem2, rsem2, ssem3, rsem3, rpair, fsem, rfwd,
):
    kv = lax.axis_index("kv")
    tp = lax.axis_index("tp")
    z = kv // 8
    xc = kv % 8
    z4 = (z + 4) % 8

    locals_ = [
        pltpu.make_async_copy(x_hbm, x_v, lsem.at[0]),
        pltpu.make_async_copy(pf_hbm, pf_v, lsem.at[1]),
        pltpu.make_async_copy(pv_hbm, pv_v, lsem.at[2]),
        pltpu.make_async_copy(acc_hbm, acc_v, lsem.at[3]),
        pltpu.make_async_copy(floor_hbm, floor_v, lsem.at[4]),
        pltpu.make_async_copy(base_hbm, base_v, lsem.at[5]),
        pltpu.make_async_copy(gain_hbm, gain_v, lsem.at[6]),
        pltpu.make_async_copy(wq_hbm, w_v.at[0], lsem.at[7]),
        pltpu.make_async_copy(wf_hbm, w_v.at[1], lsem.at[8]),
        pltpu.make_async_copy(wi_hbm, w_v.at[2], lsem.at[9]),
        pltpu.make_async_copy(wg_hbm, w_v.at[3], lsem.at[10]),
        pltpu.make_async_copy(hgain_hbm, hgain_v, lsem.at[11]),
        pltpu.make_async_copy(wo_hbm, wo_v, lsem.at[12]),
    ]
    for copy in locals_:
        copy.start()

    barrier = pltpu.get_barrier_semaphore()

    def greet(zd, xd):
        pl.semaphore_signal(barrier, inc=1, device_id={"kv": zd * 8 + xd}, device_id_type=MESH)

    for dist in (4,) + FAR_FIRST:
        for k in range(1 if dist == 0 else 0, 8):
            greet((z + dist) % 8, (xc + k) % 8)
    for k in range(1, NTP):
        pl.semaphore_signal(barrier, inc=1, device_id={"tp": (tp + k) % NTP}, device_id_type=MESH)

    locals_[0].wait()
    for b in range(8):
        block = x_v[:, :, 128 * b : 128 * (b + 1)].reshape(128, 128)
        tx1[8 * b : 8 * (b + 1)] = jnp.transpose(block).reshape(8, SEQ, 128)

    for i in range(1, 6):
        locals_[i].wait()
    fl = floor_v[...]
    row4 = lax.broadcasted_iota(jnp.int32, (PROPS, 2 * HD), 0)
    ones_row = (lax.broadcasted_iota(jnp.int32, (8, HD), 0) == 4).astype(jnp.float32)
    seq_lane = lax.broadcasted_iota(jnp.int32, (1, SEQ), 1)

    def state_step(s, c):
        count = jnp.sum(jnp.where(seq_lane == s, acc_v[...], 0), axis=1, keepdims=True)
        live = row4 < count
        f = fl + (1.0 - fl) * sigmoid(pf_v[s].astype(jnp.float32))
        k = jnp.where(live, 1.0 - f, 0.0)
        f = jnp.where(live, f, 1.0)
        v = pv_v[s].astype(jnp.float32)
        f0, f1, f2, f3 = (f[j : j + 1] for j in range(4))
        f23 = f2 * f3
        f123 = f1 * f23
        coef = jnp.concatenate(
            [k[0:1] * f123, k[1:2] * f23, k[2:3] * f3, k[3:4], f0 * f123, jnp.zeros((3, 2 * HD), jnp.float32)],
            axis=0,
        )
        high = coef.astype(jnp.bfloat16).astype(jnp.float32)
        rest = coef - high
        mid = rest.astype(jnp.bfloat16).astype(jnp.float32)
        lhs = jnp.concatenate([high, mid, rest - mid, jnp.zeros((8, 2 * HD), jnp.float32)], axis=0).astype(jnp.bfloat16)
        for h in range(2):
            cols = slice(h * HD, (h + 1) * HD)
            rows = jnp.concatenate([v[:, cols], jnp.zeros((4, HD), jnp.float32)], axis=0)
            rows = jnp.concatenate([ones_row, rows], axis=1)
            rhs = jnp.concatenate([rows] * 4, axis=0).astype(jnp.bfloat16)
            spread = lax.dot_general(
                lhs[:, cols], rhs, (((0,), (0,)), ((), ())), preferred_element_type=jnp.float32
            )
            new = spread[:, :HD] * base_v[s, h] + spread[:, HD:]
            taken_ref[s, h] = new
            s0_v[s, h] = new.astype(jnp.bfloat16)
        return c

    lax.fori_loop(0, EARLY, state_step, 0, unroll=4)

    pl.semaphore_wait(barrier, NKV - 1 + NTP - 1)

    def send_pair(tx, rx, send_sem, side):
        first = z4 * 8 + ((xc // 2 - tp + 4) % 4) * 2
        for k in range(2):
            pltpu.make_async_remote_copy(
                src_ref=tx.at[first + k], dst_ref=rx.at[kv], send_sem=send_sem, recv_sem=rpair.at[side],
                device_id={"kv": first + k}, device_id_type=MESH,
            ).start()

    def send_group(tx, rx, send_sem, recv_sem, dist):
        zd = (z + dist) % 8
        for k in range(1 if dist == 0 else 0, 8):
            d = zd * 8 + (xc + k) % 8
            pltpu.make_async_remote_copy(
                src_ref=tx.at[d], dst_ref=rx.at[kv], send_sem=send_sem, recv_sem=recv_sem.at[z],
                device_id={"kv": d}, device_id_type=MESH,
            ).start()

    def wait_group(rx, send_sem, recv_sem, dist):
        zs = (z + dist) % 8
        group = rx.at[pl.ds(0, 7)] if dist == 0 else rx.at[pl.ds(pl.multiple_of(zs * 8, 8), 8)]
        pltpu.make_async_remote_copy(
            src_ref=group, dst_ref=group, send_sem=send_sem, recv_sem=recv_sem.at[zs],
            device_id={"kv": kv}, device_id_type=MESH,
        ).wait_recv()

    def pass_on(rx, send_sem, side):
        pair = rx.at[pl.ds(z4 * 8 + ((xc // 2 + tp) % 4) * 2, 2)]
        pltpu.make_async_remote_copy(
            src_ref=pair, dst_ref=pair, send_sem=send_sem, recv_sem=rpair.at[side],
            device_id={"kv": kv}, device_id_type=MESH,
        ).wait_recv()
        copies = []
        for k in (2, 1, 3):
            copy = pltpu.make_async_remote_copy(
                src_ref=pair, dst_ref=pair, send_sem=fsem.at[side, k], recv_sem=rfwd.at[side, k],
                device_id={"tp": (tp + k) % NTP}, device_id_type=MESH,
            )
            copy.start()
            copies.append(copy)
        return copies

    def wait_far(rx, side):
        for k in (1, 3, 2):
            pair = rx.at[pl.ds(z4 * 8 + ((xc // 2 + tp - k + 4) % 4) * 2, 2)]
            pltpu.make_async_remote_copy(
                src_ref=pair, dst_ref=pair, send_sem=fsem.at[side, k], recv_sem=rfwd.at[side, k],
                device_id={"tp": (tp + k) % NTP}, device_id_type=MESH,
            ).wait_recv()

    send_pair(tx1, rx1, ssem1, 0)
    for dist in FAR_FIRST:
        send_group(tx1, rx1, ssem1, rsem1, dist)
    rx1[kv] = tx1[kv]

    lax.fori_loop(EARLY, SEQ, state_step, 0, unroll=4)
    passed = pass_on(rx1, ssem1, 0)
    for i in range(6, 11):
        locals_[i].wait()
    squares = jnp.zeros((SEQ, 128), jnp.float32)
    for n, dist in enumerate((0, 1, 7, 2, 6, 3, 5, 4)):
        zs = (z + dist) % 8
        if dist == 4:
            wait_far(rx1, 0)
        else:
            wait_group(rx1, ssem1, rsem1, dist)
        vals = rx1[pl.ds(pl.multiple_of(zs * 8, 8), 8)].astype(jnp.float32)
        squares = squares + jnp.sum(vals * vals, axis=0)
        tiles = []
        for q in range(2):
            swapped = swap_blocks([vals[4 * q + i] for i in range(4)])
            gain = gain_v[:, pl.ds(pl.multiple_of(zs * 256 + q * 128, 128), 128)]
            tiles.append(jnp.concatenate([(part * gain).astype(jnp.bfloat16) for part in swapped], axis=0))
        lhs = jnp.concatenate(tiles, axis=1)
        for i in range(4):
            w = w_v[i, pl.ds(pl.multiple_of(zs * 256, 256), 256), :]
            prod = jnp.dot(lhs, w, preferred_element_type=jnp.float32)
            if n == 0:
                pre_v[i] = prod
            else:
                pre_v[i] += prod
    lane = lax.broadcasted_iota(jnp.int32, (SEQ, 128), 1)
    scale = jnp.concatenate(
        [
            lax.rsqrt(
                jnp.sum(jnp.where(lane // F == p, squares, 0.0), axis=1, keepdims=True) / D + 1e-06
            )
            for p in range(PROPS)
        ],
        axis=0,
    )

    def pre(i):
        return (pre_v[i] * scale).astype(jnp.bfloat16).astype(jnp.float32)

    q_all = pre(0)
    q_all = q_all * sigmoid(q_all)
    f_all = fl + (1.0 - fl) * sigmoid(pre(1))
    k_all = 1.0 - f_all
    v_all = pre(2)

    def at(arr, t):
        return arr[t * SEQ : (t + 1) * SEQ]

    decay = None
    for t in range(PROPS):
        decay = at(f_all, t) if t == 0 else decay * at(f_all, t)
        for h in range(2):
            a_v[h, t * SEQ : (t + 1) * SEQ, :] = (at(q_all, t) * decay)[:, h * HD : (h + 1) * HD]
    locals_[11].wait()
    hg = hgain_v[...]
    gate = pre(3)
    gate = gate * sigmoid(gate)
    gathers = {}
    for h in range(2):
        cols = slice(h * HD, (h + 1) * HD)
        for s in range(SEQ):
            lhs = a_v[h, pl.ds(s, PROPS, stride=SEQ), :].astype(jnp.bfloat16)
            o_v[h, pl.ds(s, PROPS, stride=SEQ), :] = jnp.dot(lhs, s0_v[s, h], preferred_element_type=jnp.float32)
        for t in range(PROPS):
            weight = at(q_all, t)[:, cols]
            extra = jnp.zeros((SEQ, HD), jnp.float32)
            for j in range(t, -1, -1):
                c = jnp.sum(weight * at(k_all, j)[:, cols], axis=1, keepdims=True)
                extra = extra + c * at(v_all, j)[:, cols]
                if j:
                    weight = weight * at(f_all, j)[:, cols]
            o = o_v[h, t * SEQ : (t + 1) * SEQ, :] + extra
            norm = lax.rsqrt(jnp.mean(o * o, axis=1, keepdims=True) + 1e-05)
            mh_v[tp, h, t * SEQ : (t + 1) * SEQ, :] = (o * norm * hg * at(gate, t)[:, cols]).astype(jnp.bfloat16)
        for k in (2, 1, 3):
            gathers[k, h] = pltpu.make_async_remote_copy(
                src_ref=mh_v.at[tp, h], dst_ref=mh_v.at[tp, h], send_sem=ssem2.at[k, h], recv_sem=rsem2.at[k, h],
                device_id={"tp": (tp + k) % NTP}, device_id_type=MESH,
            )
            gathers[k, h].start()
    locals_[12].wait()

    def piece(k, cols):
        place = (tp - k + NTP) % NTP
        w = wo_v[pl.ds(pl.multiple_of(place * 256, 256), 256), cols]
        return jnp.dot(jnp.concatenate([mh_v[place, 0], mh_v[place, 1]], axis=1), w, preferred_element_type=jnp.float32)

    for k in (0, 1, 3):
        if k:
            gathers[k, 0].wait_recv()
            gathers[k, 1].wait_recv()
        for n in range(4):
            cols = slice(n * 512, (n + 1) * 512)
            if k:
                acc_o[:, cols] += piece(k, cols)
            else:
                acc_o[:, cols] = piece(k, cols)
    gathers[2, 0].wait_recv()
    gathers[2, 1].wait_recv()

    def finish(first, tiles):
        cols = pl.ds(pl.multiple_of(first * F, 128), tiles * 128)
        out = acc_o[:, cols] + piece(2, cols)
        for q in range(tiles):
            blocks = swap_blocks([out[p * SEQ : (p + 1) * SEQ, q * 128 : (q + 1) * 128] for p in range(PROPS)])
            for j in range(4):
                tx2[first + 4 * q + j] = blocks[j].astype(jnp.bfloat16)

    finish(z4 * 8 + ((xc // 2 - tp + 4) % 4) // 2 * 4, 1)
    send_pair(tx2, rx2, ssem3, 1)
    for dist in FAR_FIRST:
        finish((z + dist) % 8 * 8, 2)
        send_group(tx2, rx2, ssem3, rsem3, dist)
    rx2[kv] = tx2[kv]

    def place_group(dist):
        zs = (z + dist) % 8
        block = rx2[pl.ds(pl.multiple_of(zs * 8, 8), 8)].reshape(128, 128)
        mixed_ref[:, :, pl.ds(pl.multiple_of(zs * 128, 128), 128)] = jnp.transpose(block).reshape(
            PROPS, F, 128
        )

    passed += pass_on(rx2, ssem3, 1)
    for dist in (0, 1, 7, 2, 6, 3, 5):
        wait_group(rx2, ssem3, rsem3, dist)
        place_group(dist)
    wait_far(rx2, 1)
    place_group(4)
    for copy in passed:
        copy.wait_send()
    for copy in gathers.values():
        copy.wait_send()
    for tx, sem in ((tx1, ssem1), (tx2, ssem3)):
        sent = tx.at[pl.ds(0, NKV - 1 - 6)]
        pltpu.make_async_remote_copy(
            src_ref=sent, dst_ref=sent, send_sem=sem, recv_sem=sem,
            device_id={"kv": kv}, device_id_type=MESH,
        ).wait_send()


def tail(mixed_v, taken_v, mixed_hbm, taken_hbm, sem):
    copies = [pltpu.make_async_copy(mixed_v, mixed_hbm, sem.at[8])]
    for i in range(8):
        part = pl.ds(2 * i, 2)
        copies.append(pltpu.make_async_copy(taken_v.at[part], taken_hbm.at[part], sem.at[i]))
    for copy in copies:
        copy.start()
    for copy in copies:
        copy.wait()


def shards(hidden, norm_gain, w_query, w_forget, w_input, w_outgate, w_out, floor, head_gain, base_state, prev_forget, prev_input, accepted):
    any_spec = pl.BlockSpec(memory_space=pl.ANY)
    vmem = pl.BlockSpec(memory_space=pltpu.VMEM)
    bf, f32 = jnp.bfloat16, jnp.float32
    mixed, taken = pl.pallas_call(
        kernel,
        name="verify",
        out_shape=(
            pltpu.VMEM((PROPS, F, NKV * SEQ), bf),
            pltpu.VMEM((SEQ, 2, HD, HD), f32),
        ),
        in_specs=[any_spec] * 13,
        out_specs=(vmem, vmem),
        scratch_shapes=[
            pltpu.VMEM((PROPS, F, NKV * SEQ), bf),
            pltpu.VMEM((1, D), f32),
            pltpu.VMEM((4, D, 256), bf),
            pltpu.VMEM((1024, D), bf),
            pltpu.VMEM((1, 256), f32),
            pltpu.VMEM((1, HD), f32),
            pltpu.VMEM((SEQ, 2, HD, HD), f32),
            pltpu.VMEM((SEQ, PROPS, 256), bf),
            pltpu.VMEM((SEQ, PROPS, 256), bf),
            pltpu.VMEM((1, SEQ), jnp.int32),
            pltpu.VMEM((SEQ, 2, HD, HD), bf),
            pltpu.VMEM((NKV, SEQ, 128), bf),
            pltpu.VMEM((NKV, SEQ, 128), bf),
            pltpu.VMEM((4, ROWS, 256), f32),
            pltpu.VMEM((2, ROWS, HD), f32),
            pltpu.VMEM((2, ROWS, HD), f32),
            pltpu.VMEM((NTP, 2, ROWS, HD), bf),
            pltpu.VMEM((NKV, SEQ, 128), bf),
            pltpu.VMEM((NKV, SEQ, 128), bf),
            pltpu.VMEM((ROWS, D), f32),
            pltpu.SemaphoreType.DMA((13,)),
            pltpu.SemaphoreType.DMA,
            pltpu.SemaphoreType.DMA((8,)),
            pltpu.SemaphoreType.DMA((NTP, 2)),
            pltpu.SemaphoreType.DMA((NTP, 2)),
            pltpu.SemaphoreType.DMA,
            pltpu.SemaphoreType.DMA((8,)),
            pltpu.SemaphoreType.DMA((2,)),
            pltpu.SemaphoreType.DMA((2, NTP)),
            pltpu.SemaphoreType.DMA((2, NTP)),
        ],
        compiler_params=pltpu.CompilerParams(collective_id=0, has_side_effects=True),
    )(
        jnp.transpose(hidden, (1, 2, 0)),
        norm_gain.reshape(1, -1),
        w_query, w_forget, w_input, w_outgate, w_out,
        floor.reshape(1, -1),
        head_gain.reshape(1, -1),
        base_state, prev_forget, prev_input,
        accepted.reshape(1, -1),
    )
    mixed, taken = pl.pallas_call(
        tail,
        name="place",
        out_shape=(
            jax.ShapeDtypeStruct((PROPS, F, NKV * SEQ), bf),
            jax.ShapeDtypeStruct((SEQ, 2, HD, HD), f32),
        ),
        in_specs=[vmem] * 2,
        out_specs=(any_spec,) * 2,
        scratch_shapes=[pltpu.SemaphoreType.DMA((9,))],
    )(pltpu.with_memory_space_constraint(mixed, pltpu.VMEM), pltpu.with_memory_space_constraint(taken, pltpu.VMEM))
    return jnp.transpose(mixed, (2, 0, 1)), taken


def solution(mesh):
    in_specs = (
        P(None, None, "kv"), P(), P(None, "tp"), P(None, "tp"), P(None, "tp"), P(None, "tp"), P(), P("tp"), P(),
        P("kv", "tp", None, None), P("kv", None, "tp"), P("kv", None, "tp"), P("kv"),
    )
    out_specs = (P(None, None, "kv"), P("kv", "tp", None, None))
    return jax.shard_map(shards, mesh=mesh, in_specs=in_specs, out_specs=out_specs, check_vma=False)
```

```python
import functools

import jax
import jax.numpy as jnp
from jax import lax
from jax.experimental import pallas as pl
from jax.experimental.pallas import tpu as pltpu
from jax.sharding import PartitionSpec as P

D = 2048
HD = 128
PROPS = 4
NKV = 64
NTP = 4
SEQ = 16
ROWS = SEQ * PROPS
F = D // NKV
EARLY = 4
MESH = pl.DeviceIdType.MESH
ORDER = (0, 1, 7, 2, 6, 3, 5, 4)
RELAYED = (4, 3, 5)
DIRECT = ((2, 6, 1, 7, 0), (3, 5, 2, 6, 1, 7, 0))
HOLD = {3: 0, 5: 1, 4: 2}


def swap_blocks(parts):
    lane = lax.broadcasted_iota(jnp.int32, parts[0].shape, parts[0].ndim - 1)
    axis = parts[0].ndim - 1
    low = lane < 64
    even = (lane // 32) % 2 == 0
    a0, a1, a2, a3 = parts
    c0 = jnp.where(low, a0, pltpu.roll(a2, 64, axis))
    c2 = jnp.where(low, pltpu.roll(a0, 64, axis), a2)
    c1 = jnp.where(low, a1, pltpu.roll(a3, 64, axis))
    c3 = jnp.where(low, pltpu.roll(a1, 64, axis), a3)
    b0 = jnp.where(even, c0, pltpu.roll(c1, 32, axis))
    b1 = jnp.where(even, pltpu.roll(c0, 96, axis), c1)
    b2 = jnp.where(even, c2, pltpu.roll(c3, 32, axis))
    b3 = jnp.where(even, pltpu.roll(c2, 96, axis), c3)
    return b0, b1, b2, b3


def sigmoid(x):
    return jax.nn.sigmoid(x)


def kernel(
    x_hbm, gain_hbm, wq_hbm, wf_hbm, wi_hbm, wg_hbm, wo_hbm, floor_hbm, hgain_hbm,
    base_hbm, pf_hbm, pv_hbm, acc_hbm,
    mixed_ref, taken_ref,
    x_v, gain_v, w_v, wo_v, floor_v, hgain_v, base_v, pf_v, pv_v, acc_v,
    s0_v, tx1, rx1, pre_v, a_v, o_v, mh_v, tx2, rx2,
    acc_o,
    hold,
    lsem, ssem, rsem, hsem, fsem, gsem, psem, qsem, ssem2, rsem2,
):
    kv = lax.axis_index("kv")
    tp = lax.axis_index("tp")
    z = kv // 8
    xc = kv % 8
    mine = xc % 2
    xr_base = xc // 2
    turn = [(tp + 2 * mine + part) % 4 for part in range(2)]
    xd = [(xr_base + 4 - turn[part]) % 4 for part in range(2)]

    barrier = pltpu.get_barrier_semaphore()
    locals_ = [
        pltpu.make_async_copy(x_hbm, x_v, lsem.at[0]),
        pltpu.make_async_copy(pf_hbm, pf_v, lsem.at[1]),
        pltpu.make_async_copy(pv_hbm, pv_v, lsem.at[2]),
        pltpu.make_async_copy(acc_hbm, acc_v, lsem.at[3]),
        pltpu.make_async_copy(floor_hbm, floor_v, lsem.at[4]),
        pltpu.make_async_copy(base_hbm, base_v, lsem.at[5]),
        pltpu.make_async_copy(gain_hbm, gain_v, lsem.at[6]),
        pltpu.make_async_copy(wq_hbm, w_v.at[0], lsem.at[7]),
        pltpu.make_async_copy(wf_hbm, w_v.at[1], lsem.at[8]),
        pltpu.make_async_copy(wi_hbm, w_v.at[2], lsem.at[9]),
        pltpu.make_async_copy(wg_hbm, w_v.at[3], lsem.at[10]),
        pltpu.make_async_copy(hgain_hbm, hgain_v, lsem.at[11]),
        pltpu.make_async_copy(wo_hbm, wo_v, lsem.at[12]),
    ]
    locals_[0].start()


    def greet(where):
        pl.semaphore_signal(barrier, inc=1, device_id=where, device_id_type=MESH)

    for dist in RELAYED:
        greet({"kv": (z + dist) % 8 * 8 + xc})
    for part in range(2):
        for r in (2, 1, 3, 0):
            for m in range(2):
                core = (mine + m) % 2
                where = {"kv": z * 8 + (xr_base + r) % 4 * 2 + core, "tp": (r + 2 * core + 4 - part) % 4}
                if r == 0 and m == 0:
                    pl.when(turn[part] != 0)(functools.partial(greet, where))
                else:
                    greet(where)
    for dist in DIRECT[0]:
        for k in range(1 if dist == 0 else 0, 8):
            greet({"kv": (z + dist) % 8 * 8 + (xc + 4 + k) % 8 if dist else z * 8 + (xc + k) % 8})
    for k in range(1, NTP):
        greet({"tp": (tp + k) % NTP})

    for copy in locals_[1:]:
        copy.start()

    locals_[0].wait()
    for b in range(8):
        block = x_v[:, :, 128 * b : 128 * (b + 1)].reshape(128, 128)
        tx1[8 * b : 8 * (b + 1)] = jnp.transpose(block).reshape(8, SEQ, 128)

    for i in range(1, 6):
        locals_[i].wait()
    fl = floor_v[...]
    row4 = lax.broadcasted_iota(jnp.int32, (PROPS, 2 * HD), 0)
    a_v[...] = jnp.zeros_like(a_v)
    ones_row = (lax.broadcasted_iota(jnp.int32, (8, HD), 0) == 4).astype(jnp.float32)
    seq_lane = lax.broadcasted_iota(jnp.int32, (1, SEQ), 1)

    def state_step(s, c):
        count = jnp.sum(jnp.where(seq_lane == s, acc_v[...], 0), axis=1, keepdims=True)
        live = row4 < count
        f = fl + (1.0 - fl) * sigmoid(pf_v[s].astype(jnp.float32))
        k = jnp.where(live, 1.0 - f, 0.0)
        f = jnp.where(live, f, 1.0)
        v = pv_v[s].astype(jnp.float32)
        f0, f1, f2, f3 = (f[j : j + 1] for j in range(4))
        f23 = f2 * f3
        f123 = f1 * f23
        coef = jnp.concatenate(
            [k[0:1] * f123, k[1:2] * f23, k[2:3] * f3, k[3:4], f0 * f123, jnp.zeros((3, 2 * HD), jnp.float32)],
            axis=0,
        )
        high = coef.astype(jnp.bfloat16).astype(jnp.float32)
        rest = coef - high
        mid = rest.astype(jnp.bfloat16).astype(jnp.float32)
        lhs = jnp.concatenate([high, mid, rest - mid, jnp.zeros((8, 2 * HD), jnp.float32)], axis=0).astype(jnp.bfloat16)
        for h in range(2):
            cols = slice(h * HD, (h + 1) * HD)
            rows = jnp.concatenate([v[:, cols], jnp.zeros((4, HD), jnp.float32)], axis=0)
            rows = jnp.concatenate([ones_row, rows], axis=1)
            rhs = jnp.concatenate([rows] * 4, axis=0).astype(jnp.bfloat16)
            spread = lax.dot_general(
                lhs[:, cols], rhs, (((0,), (0,)), ((), ())), preferred_element_type=jnp.float32
            )
            new = spread[:, :HD] * base_v[s, h] + spread[:, HD:]
            taken_ref[s, h] = new
            s0_v[s, cols, :] = new.astype(jnp.bfloat16)
        return c

    lax.fori_loop(0, EARLY, state_step, 0, unroll=4)

    others = (turn[0] + 3) // 4 + (turn[1] + 3) // 4
    pl.semaphore_wait(barrier, 8 * len(DIRECT[0]) - 1 + len(RELAYED) + NTP - 1 + 14 + others)


    def move(src, dst, send_sem, recv_sem, where):
        return pltpu.make_async_remote_copy(
            src_ref=src, dst_ref=dst, send_sem=send_sem, recv_sem=recv_sem, device_id=where, device_id_type=MESH
        )

    def send_relayed(dist):
        zd = (z + dist) % 8
        slot = HOLD[8 - dist]
        move(
            tx1.at[pl.ds(zd * 8 + xd[slot // 2] * 2, 2)], hold.at[slot], ssem.at[0], hsem.at[slot // 2],
            {"kv": zd * 8 + xc},
        ).start()

    pair = (z + 4) % 8 * 8 + (xr_base + 4 - tp) % 4 * 2

    def send_pair():
        for k in range(2):
            move(tx2.at[pair + k], rx2.at[7, xc], ssem.at[1], psem, {"kv": pair + k}).start()

    def send_direct(side, dist):
        tx, rx = ((tx1, rx1), (tx2, rx2))[side]
        zd = (z + dist) % 8
        slot = ORDER.index((8 - dist) % 8)
        for k in range(1 if dist == 0 else 0, 8):
            d = zd * 8 + (xc + k) % 8
            move(tx.at[d], rx.at[slot, xc], ssem.at[side], rsem.at[side, slot], {"kv": d}).start()

    def pass_on(part):
        held = hold.at[pl.ds(2 * part, 2 - part)]
        to = rx1.at[pl.ds(5 + 2 * part, 2 - part)]
        move(held, held, ssem.at[0], hsem.at[part], {"kv": kv}).wait_recv()
        for m in range(2):
            core = (mine + m) % 2
            for k in (2, 1, 3, 0):
                copy = move(
                    held.at[:, core], to.at[:, xc], fsem.at[part], gsem.at[part],
                    {"kv": z * 8 + xd[part] * 2 + core, "tp": (tp + k) % NTP},
                )
                if m == 0 and k == 0:
                    pl.when(turn[part] != 0)(copy.start)

                    @pl.when(turn[part] == 0)
                    def _():
                        for b in range(2 - part):
                            rx1[5 + 2 * part + b, xc] = hold[2 * part + b, core]
                else:
                    copy.start()

    def all_passed(part):
        to = rx1.at[pl.ds(5 + 2 * part, 2 - part)]
        less = rx1.at[pl.ds(5 + 2 * part, 2 - part), pl.ds(0, 7)]
        return [move(ref, ref, fsem.at[part], gsem.at[part], {"kv": kv}) for ref in (to, less)]

    def wait_passed(part):
        full, less = all_passed(part)
        pl.when(turn[part] != 0)(full.wait_recv)
        pl.when(turn[part] == 0)(less.wait_recv)

    def pair_at(k):
        return rx2.at[7, pl.ds((xr_base + tp + k) % 4 * 2, 2)]

    def pass_pair():
        move(pair_at(0), pair_at(0), ssem.at[1], psem, {"kv": kv}).wait_recv()
        copies = [
            move(pair_at(0), pair_at(0), qsem.at[0, k], qsem.at[1, k], {"tp": (tp + k) % NTP}) for k in (2, 1, 3)
        ]
        for copy in copies:
            copy.start()
        return copies

    def wait_direct(side, slot):
        rx = (rx1, rx2)[side]
        group = rx.at[slot, pl.ds(0, 7 if slot == 0 else 8)]
        move(group, group, ssem.at[side], rsem.at[side, slot], {"kv": kv}).wait_recv()

    for dist in RELAYED:
        send_relayed(dist)
    rx1[0, xc] = tx1[kv]

    lax.fori_loop(EARLY, SEQ, state_step, 0, unroll=4)
    for dist in DIRECT[0]:
        send_direct(0, dist)
    pass_on(0)
    pass_on(1)
    for i in range(6, 11):
        locals_[i].wait()
    squares = jnp.zeros((SEQ, 128), jnp.float32)

    def take(n):
        zs = (z + ORDER[n]) % 8
        vals = rx1[n].astype(jnp.float32)
        tiles = []
        for q in range(2):
            swapped = swap_blocks([vals[4 * q + i] for i in range(4)])
            gain = gain_v[:, pl.ds(pl.multiple_of(zs * 256 + q * 128, 128), 128)]
            tiles.append(jnp.concatenate([(part * gain).astype(jnp.bfloat16) for part in swapped], axis=0))
        lhs = jnp.concatenate(tiles, axis=1)
        prods = [
            jnp.dot(lhs, w_v[i, pl.ds(pl.multiple_of(zs * 256, 256), 256), :], preferred_element_type=jnp.float32)
            for i in range(4)
        ]
        return jnp.sum(vals * vals, axis=0), prods

    for n in range(5):
        wait_direct(0, n)
        part, prods = take(n)
        squares = squares + part
        for i in range(4):
            if n == 0:
                pre_v[i] = prods[i]
            else:
                pre_v[i] += prods[i]
    wait_passed(0)
    wait_passed(1)
    last = [take(n) for n in (5, 6, 7)]
    squares = squares + last[0][0] + last[1][0] + last[2][0]
    sums = [pre_v[i] + (last[0][1][i] + last[1][1][i] + last[2][1][i]) for i in range(4)]
    lane = lax.broadcasted_iota(jnp.int32, (SEQ, 128), 1)
    scale = jnp.concatenate(
        [
            lax.rsqrt(
                jnp.sum(jnp.where(lane // F == p, squares, 0.0), axis=1, keepdims=True) / D + 1e-06
            )
            for p in range(PROPS)
        ],
        axis=0,
    )

    def pre(i):
        return (sums[i] * scale).astype(jnp.bfloat16).astype(jnp.float32)

    q_all = pre(0)
    q_all = q_all * sigmoid(q_all)
    f_all = fl + (1.0 - fl) * sigmoid(pre(1))
    k_all = 1.0 - f_all
    v_all = pre(2)

    def at(arr, t):
        return arr[t * SEQ : (t + 1) * SEQ]

    decay = None
    for t in range(PROPS):
        decay = at(f_all, t) if t == 0 else decay * at(f_all, t)
        scaled = at(q_all, t) * decay
        for h in range(2):
            a_v[h, pl.ds(4 * h + t, SEQ, stride=8), :] = scaled[:, h * HD : (h + 1) * HD]
    for s in range(SEQ):
        lhs = jnp.concatenate([a_v[0, 8 * s : 8 * s + 8], a_v[1, 8 * s : 8 * s + 8]], axis=1).astype(jnp.bfloat16)
        o_v[8 * s : 8 * s + 8] = jnp.dot(lhs, s0_v[s], preferred_element_type=jnp.float32)
    locals_[11].wait()
    hg = hgain_v[...]
    gate = pre(3)
    gate = gate * sigmoid(gate)
    gathers = {}
    for h in range(2):
        cols = slice(h * HD, (h + 1) * HD)
        for t in range(PROPS):
            weight = at(q_all, t)[:, cols]
            o = o_v[pl.ds(4 * h + t, SEQ, stride=8), :]
            for j in range(t, -1, -1):
                o = o + jnp.sum(weight * at(k_all, j)[:, cols], axis=1, keepdims=True) * at(v_all, j)[:, cols]
                if j:
                    weight = weight * at(f_all, j)[:, cols]
            norm = lax.rsqrt(jnp.mean(o * o, axis=1, keepdims=True) + 1e-05)
            mh_v[tp, h, t * SEQ : (t + 1) * SEQ, :] = (o * norm * hg * at(gate, t)[:, cols]).astype(jnp.bfloat16)
        for k in (2, 1, 3):
            gathers[k, h] = pltpu.make_async_remote_copy(
                src_ref=mh_v.at[tp, h], dst_ref=mh_v.at[tp, h], send_sem=ssem2.at[k, h], recv_sem=rsem2.at[k, h],
                device_id={"tp": (tp + k) % NTP}, device_id_type=MESH,
            )
            gathers[k, h].start()
    locals_[12].wait()

    def piece(k, cols):
        place = (tp - k + NTP) % NTP
        w = wo_v[pl.ds(pl.multiple_of(place * 256, 256), 256), cols]
        return jnp.dot(jnp.concatenate([mh_v[place, 0], mh_v[place, 1]], axis=1), w, preferred_element_type=jnp.float32)

    for k in (0, 1, 3):
        if k:
            gathers[k, 0].wait_recv()
            gathers[k, 1].wait_recv()
        for n in range(4):
            cols = slice(n * 512, (n + 1) * 512)
            if k:
                acc_o[:, cols] += piece(k, cols)
            else:
                acc_o[:, cols] = piece(k, cols)
    gathers[2, 0].wait_recv()
    gathers[2, 1].wait_recv()

    def product(first, tiles):
        cols = pl.ds(pl.multiple_of(first * F, 128), tiles * 128)
        return acc_o[:, cols] + piece(2, cols)

    def blocks_of(out):
        found = []
        for q in range(out.shape[1] // 128):
            parts = [out[p * SEQ : (p + 1) * SEQ, q * 128 : (q + 1) * 128] for p in range(PROPS)]
            found += [part.astype(jnp.bfloat16) for part in swap_blocks(parts)]
        return found

    chunks = [(pair // 4 * 4, 1)] + [((z + dist) % 8 * 8, 2) for dist in DIRECT[1]]
    outs = [product(*chunks[0]), product(*chunks[1])]
    ready = blocks_of(outs[0])
    for n, (first, _) in enumerate(chunks):
        if n + 2 < len(chunks):
            outs.append(product(*chunks[n + 2]))
        later = blocks_of(outs[n + 1]) if n + 1 < len(chunks) else None
        for j, block in enumerate(ready):
            tx2[first + j] = block
        if n == 0:
            send_pair()
        else:
            send_direct(1, DIRECT[1][n - 1])
        ready = later
    rx2[0, xc] = tx2[kv]
    passed = pass_pair()

    def place(n):
        mixed_ref[:, :, pl.ds(pl.multiple_of((z + ORDER[n]) % 8 * 128, 128), 128)] = jnp.transpose(
            rx2[n].reshape(128, 128)
        ).reshape(PROPS, F, 128)

    for n in (5, 6, 3, 4, 1, 2, 0):
        wait_direct(1, n)
        place(n)
    for k in (1, 3, 2):
        move(pair_at(4 - k), pair_at(4 - k), qsem.at[0, k], qsem.at[1, k], {"tp": tp}).wait_recv()
    place(7)
    for side, count in ((0, 8 * len(DIRECT[0]) - 1 + 6), (1, 8 * len(DIRECT[1]) - 1 + 2)):
        sent = (tx1, tx2)[side].at[pl.ds(0, count)]
        move(sent, sent, ssem.at[side], psem, {"kv": kv}).wait_send()
    for part in range(2):
        full, less = all_passed(part)
        pl.when(turn[part] != 0)(full.wait_send)
        pl.when(turn[part] == 0)(less.wait_send)
    for copy in passed:
        copy.wait_send()
    for copy in gathers.values():
        copy.wait_send()


def tail(mixed_v, taken_v, mixed_hbm, taken_hbm, sem):
    copies = [pltpu.make_async_copy(mixed_v, mixed_hbm, sem.at[8])]
    for i in range(8):
        part = pl.ds(2 * i, 2)
        copies.append(pltpu.make_async_copy(taken_v.at[part], taken_hbm.at[part], sem.at[i]))
    for copy in copies:
        copy.start()
    for copy in copies:
        copy.wait()


def shards(hidden, norm_gain, w_query, w_forget, w_input, w_outgate, w_out, floor, head_gain, base_state, prev_forget, prev_input, accepted):
    any_spec = pl.BlockSpec(memory_space=pl.ANY)
    vmem = pl.BlockSpec(memory_space=pltpu.VMEM)
    bf, f32 = jnp.bfloat16, jnp.float32
    mixed, taken = pl.pallas_call(
        kernel,
        name="verify",
        out_shape=(
            pltpu.VMEM((PROPS, F, NKV * SEQ), bf),
            pltpu.VMEM((SEQ, 2, HD, HD), f32),
        ),
        in_specs=[any_spec] * 13,
        out_specs=(vmem, vmem),
        scratch_shapes=[
            pltpu.VMEM((PROPS, F, NKV * SEQ), bf),
            pltpu.VMEM((1, D), f32),
            pltpu.VMEM((4, D, 256), bf),
            pltpu.VMEM((1024, D), bf),
            pltpu.VMEM((1, 256), f32),
            pltpu.VMEM((1, HD), f32),
            pltpu.VMEM((SEQ, 2, HD, HD), f32),
            pltpu.VMEM((SEQ, PROPS, 256), bf),
            pltpu.VMEM((SEQ, PROPS, 256), bf),
            pltpu.VMEM((1, SEQ), jnp.int32),
            pltpu.VMEM((SEQ, 2 * HD, HD), bf),
            pltpu.VMEM((NKV, SEQ, 128), bf),
            pltpu.VMEM((8, 8, SEQ, 128), bf),
            pltpu.VMEM((4, ROWS, 256), f32),
            pltpu.VMEM((2, 8 * SEQ, HD), f32),
            pltpu.VMEM((8 * SEQ, HD), f32),
            pltpu.VMEM((NTP, 2, ROWS, HD), bf),
            pltpu.VMEM((NKV, SEQ, 128), bf),
            pltpu.VMEM((8, 8, SEQ, 128), bf),
            pltpu.VMEM((ROWS, D), f32),
            pltpu.VMEM((3, 2, SEQ, 128), bf),
            pltpu.SemaphoreType.DMA((13,)),
            pltpu.SemaphoreType.DMA((2,)),
            pltpu.SemaphoreType.DMA((2, 7)),
            pltpu.SemaphoreType.DMA((2,)),
            pltpu.SemaphoreType.DMA((2,)),
            pltpu.SemaphoreType.DMA((2,)),
            pltpu.SemaphoreType.DMA,
            pltpu.SemaphoreType.DMA((2, NTP)),
            pltpu.SemaphoreType.DMA((NTP, 2)),
            pltpu.SemaphoreType.DMA((NTP, 2)),
        ],
        compiler_params=pltpu.CompilerParams(collective_id=0, has_side_effects=True),
    )(
        jnp.transpose(hidden, (1, 2, 0)),
        norm_gain.reshape(1, -1),
        w_query, w_forget, w_input, w_outgate, w_out,
        floor.reshape(1, -1),
        head_gain.reshape(1, -1),
        base_state, prev_forget, prev_input,
        accepted.reshape(1, -1),
    )
    mixed, taken = pl.pallas_call(
        tail,
        name="place",
        out_shape=(
            jax.ShapeDtypeStruct((PROPS, F, NKV * SEQ), bf),
            jax.ShapeDtypeStruct((SEQ, 2, HD, HD), f32),
        ),
        in_specs=[vmem] * 2,
        out_specs=(any_spec,) * 2,
        scratch_shapes=[pltpu.SemaphoreType.DMA((9,))],
    )(pltpu.with_memory_space_constraint(mixed, pltpu.VMEM), pltpu.with_memory_space_constraint(taken, pltpu.VMEM))
    return jnp.transpose(mixed, (2, 0, 1)), taken


def solution(mesh):
    in_specs = (
        P(None, None, "kv"), P(), P(None, "tp"), P(None, "tp"), P(None, "tp"), P(None, "tp"), P(), P("tp"), P(),
        P("kv", "tp", None, None), P("kv", None, "tp"), P("kv", None, "tp"), P("kv"),
    )
    out_specs = (P(None, None, "kv"), P("kv", "tp", None, None))
    return jax.shard_map(shards, mesh=mesh, in_specs=in_specs, out_specs=out_specs, check_vma=False)
```

```python
import functools

import jax
import jax.numpy as jnp
from jax import lax
from jax.experimental import pallas as pl
from jax.experimental.pallas import tpu as pltpu
from jax.sharding import PartitionSpec as P

D = 2048
HD = 128
PROPS = 4
NKV = 64
NTP = 4
SEQ = 16
ROWS = SEQ * PROPS
F = D // NKV
EARLY = 4
MESH = pl.DeviceIdType.MESH
ORDER = (0, 1, 7, 2, 6, 3, 5, 4)
RELAYED = (4, 3, 5)
DIRECT = (2, 6, 1, 7, 0)
UNITS = tuple(sorted(((zt, q) for zt in range(8) for q in range(2)), key=lambda u: (min(u[0], 4) + 1.2 * u[1], u)))
HOLD = {3: 0, 5: 1, 4: 2}


def swap_blocks(parts):
    lane = lax.broadcasted_iota(jnp.int32, parts[0].shape, parts[0].ndim - 1)
    axis = parts[0].ndim - 1
    low = lane < 64
    even = (lane // 32) % 2 == 0
    a0, a1, a2, a3 = parts
    c0 = jnp.where(low, a0, pltpu.roll(a2, 64, axis))
    c2 = jnp.where(low, pltpu.roll(a0, 64, axis), a2)
    c1 = jnp.where(low, a1, pltpu.roll(a3, 64, axis))
    c3 = jnp.where(low, pltpu.roll(a1, 64, axis), a3)
    b0 = jnp.where(even, c0, pltpu.roll(c1, 32, axis))
    b1 = jnp.where(even, pltpu.roll(c0, 96, axis), c1)
    b2 = jnp.where(even, c2, pltpu.roll(c3, 32, axis))
    b3 = jnp.where(even, pltpu.roll(c2, 96, axis), c3)
    return b0, b1, b2, b3


def sigmoid(x):
    return jax.nn.sigmoid(x)


def kernel(
    x_hbm, gain_hbm, wq_hbm, wf_hbm, wi_hbm, wg_hbm, wo_hbm, floor_hbm, hgain_hbm,
    base_hbm, pf_hbm, pv_hbm, acc_hbm,
    mixed_ref, taken_ref,
    x_v, small_v, w_v, wo_v, base_v, pfv_v, acc_v,
    s0_v, tx1, rx1, pre_v, a_v, o_v, mh_v, tx2, rx2,
    acc_o,
    hold,
    lsem, ssem, rsem, hsem, fsem, gsem, osem, asem, bsem,
):
    kv = lax.axis_index("kv")
    tp = lax.axis_index("tp")
    z = kv // 8
    xc = kv % 8
    mine = xc % 2
    xr_base = xc // 2
    turn = [(tp + 2 * mine + part) % 4 for part in range(2)]
    xd = [(xr_base + 4 - turn[part]) % 4 for part in range(2)]

    barrier = pltpu.get_barrier_semaphore()
    def local(src, dst, n):
        return pltpu.make_async_copy(src, dst, lsem.at[n])

    small = ((gain_hbm, 0, D), (floor_hbm, D, 256), (hgain_hbm, D + 256, HD))
    locals_ = [
        local(x_hbm, x_v, 0),
        local(pf_hbm, pfv_v.at[0], 1),
        local(pv_hbm, pfv_v.at[1], 1),
        local(acc_hbm, acc_v, 2),
        *(local(ref, small_v.at[:, pl.ds(at, n)], 3) for ref, at, n in small),
        local(base_hbm, base_v, 4),
        *(local(ref, w_v.at[i], 5) for i, ref in enumerate((wq_hbm, wf_hbm, wi_hbm, wg_hbm))),
        local(wo_hbm, wo_v, 6),
    ]
    whole = [x_v, pfv_v, acc_v, small_v, base_v, w_v, wo_v]

    def wait_local(n):
        local(whole[n], whole[n], n).wait()

    locals_[0].start()


    def greet(where):
        pl.semaphore_signal(barrier, inc=1, device_id=where, device_id_type=MESH)

    for dist in RELAYED:
        greet({"kv": (z + dist) % 8 * 8 + xc})
    for part in range(2):
        for r in (2, 1, 3, 0):
            for m in range(2):
                core = (mine + m) % 2
                where = {"kv": z * 8 + (xr_base + r) % 4 * 2 + core, "tp": (r + 2 * core + 4 - part) % 4}
                if r == 0 and m == 0:
                    pl.when(turn[part] != 0)(functools.partial(greet, where))
                else:
                    greet(where)
    for dist in DIRECT:
        for k in range(1 if dist == 0 else 0, 8):
            greet({"kv": (z + dist) % 8 * 8 + (xc + 4 + k) % 8 if dist else z * 8 + (xc + k) % 8})
    for k in range(1, NTP):
        greet({"tp": (tp + k) % NTP})

    for copy in locals_[1:]:
        copy.start()

    wait_local(0)
    for b in range(8):
        block = x_v[:, :, 128 * b : 128 * (b + 1)].reshape(128, 128)
        tx1[8 * b : 8 * (b + 1)] = jnp.transpose(block).reshape(8, SEQ, 128)

    for n in range(1, 5):
        wait_local(n)
    fl = small_v[:, D : D + 256]
    row4 = lax.broadcasted_iota(jnp.int32, (PROPS, 2 * HD), 0)
    a_v[...] = jnp.zeros_like(a_v)
    ones_row = (lax.broadcasted_iota(jnp.int32, (8, HD), 0) == 4).astype(jnp.float32)
    seq_lane = lax.broadcasted_iota(jnp.int32, (1, SEQ), 1)

    def state_step(s, c):
        count = jnp.sum(jnp.where(seq_lane == s, acc_v[...], 0), axis=1, keepdims=True)
        live = row4 < count
        f = fl + (1.0 - fl) * sigmoid(pfv_v[0, s].astype(jnp.float32))
        k = jnp.where(live, 1.0 - f, 0.0)
        f = jnp.where(live, f, 1.0)
        v = pfv_v[1, s].astype(jnp.float32)
        f0, f1, f2, f3 = (f[j : j + 1] for j in range(4))
        f23 = f2 * f3
        f123 = f1 * f23
        coef = jnp.concatenate(
            [k[0:1] * f123, k[1:2] * f23, k[2:3] * f3, k[3:4], f0 * f123, jnp.zeros((3, 2 * HD), jnp.float32)],
            axis=0,
        )
        high = coef.astype(jnp.bfloat16).astype(jnp.float32)
        rest = coef - high
        mid = rest.astype(jnp.bfloat16).astype(jnp.float32)
        lhs = jnp.concatenate([high, mid, rest - mid, jnp.zeros((8, 2 * HD), jnp.float32)], axis=0).astype(jnp.bfloat16)
        for h in range(2):
            cols = slice(h * HD, (h + 1) * HD)
            rows = jnp.concatenate([v[:, cols], jnp.zeros((4, HD), jnp.float32)], axis=0)
            rows = jnp.concatenate([ones_row, rows], axis=1)
            rhs = jnp.concatenate([rows] * 4, axis=0).astype(jnp.bfloat16)
            spread = lax.dot_general(
                lhs[:, cols], rhs, (((0,), (0,)), ((), ())), preferred_element_type=jnp.float32
            )
            new = spread[:, :HD] * base_v[s, h] + spread[:, HD:]
            taken_ref[s, h] = new
            s0_v[s, cols, :] = new.astype(jnp.bfloat16)
        return c

    lax.fori_loop(0, EARLY, state_step, 0, unroll=4)

    others = (turn[0] + 3) // 4 + (turn[1] + 3) // 4
    pl.semaphore_wait(barrier, 8 * len(DIRECT) - 1 + len(RELAYED) + NTP - 1 + 14 + others)


    def move(src, dst, send_sem, recv_sem, where):
        return pltpu.make_async_remote_copy(
            src_ref=src, dst_ref=dst, send_sem=send_sem, recv_sem=recv_sem, device_id=where, device_id_type=MESH
        )

    def send_relayed(dist):
        zd = (z + dist) % 8
        slot = HOLD[8 - dist]
        move(
            tx1.at[pl.ds(zd * 8 + xd[slot // 2] * 2, 2)], hold.at[slot], ssem.at[0], hsem.at[slot // 2],
            {"kv": zd * 8 + xc},
        ).start()

    def send_direct(side, dist):
        tx, rx = ((tx1, rx1), (tx2, rx2))[side]
        zd = (z + dist) % 8
        slot = ORDER.index((8 - dist) % 8)
        for k in range(1 if dist == 0 else 0, 8):
            d = zd * 8 + (xc + k) % 8
            move(tx.at[d], rx.at[slot, xc], ssem.at[side], rsem.at[(slot + 1) // 2], {"kv": d}).start()

    def other(k):
        return tp if k == 3 else k + (k - tp + 4) // 4

    def pass_on(part):
        held = hold.at[pl.ds(2 * part, 2 - part)]
        to = rx1.at[pl.ds(5 + 2 * part, 2 - part)]
        move(held, held, ssem.at[0], hsem.at[part], {"kv": kv}).wait_recv()
        for m in range(2):
            core = (mine + m) % 2
            for k in range(NTP):
                copy = move(
                    held.at[:, core], to.at[:, xc], fsem, gsem,
                    {"kv": z * 8 + xd[part] * 2 + core, "tp": other(k)},
                )
                if m == 0 and k == 3:
                    pl.when(turn[part] != 0)(copy.start)

                    @pl.when(turn[part] == 0)
                    def _():
                        for b in range(2 - part):
                            rx1[5 + 2 * part + b, xc] = hold[2 * part + b, core]
                else:
                    copy.start()

    def all_passed(wait):
        for when, blocks in ((turn[0] == 0, 22), (turn[1] == 0, 23), (turn[0] * turn[1] != 0, 24)):
            some = tx1.at[pl.ds(0, blocks)]
            pl.when(when)(functools.partial(wait, move(some, some, fsem, gsem, {"kv": kv})))

    def wait_direct(part):
        group = rx1.at[pl.ds(1, 2)] if part else rx1.at[0, pl.ds(0, 7)]
        move(group, group, ssem.at[0], rsem.at[part], {"kv": kv}).wait_recv()

    for dist in RELAYED:
        send_relayed(dist)
    rx1[0, xc] = tx1[kv]

    lax.fori_loop(EARLY, SEQ, state_step, 0, unroll=4)
    for dist in DIRECT:
        send_direct(0, dist)
    pass_on(0)
    pass_on(1)
    wait_local(5)
    squares = jnp.zeros((SEQ, 128), jnp.float32)

    def take(n):
        zs = (z + ORDER[n]) % 8
        vals = rx1[n].astype(jnp.float32)
        tiles = []
        for q in range(2):
            swapped = swap_blocks([vals[4 * q + i] for i in range(4)])
            gain = small_v[:, pl.ds(pl.multiple_of(zs * 256 + q * 128, 128), 128)]
            tiles.append(jnp.concatenate([(part * gain).astype(jnp.bfloat16) for part in swapped], axis=0))
        lhs = jnp.concatenate(tiles, axis=1)
        prods = [
            jnp.dot(lhs, w_v[i, pl.ds(pl.multiple_of(zs * 256, 256), 256), :], preferred_element_type=jnp.float32)
            for i in range(4)
        ]
        return jnp.sum(vals * vals, axis=0), prods

    for n in range(5):
        if n in (0, 1, 3):
            wait_direct((n + 1) // 2)
        part, prods = take(n)
        squares = squares + part
        for i in range(4):
            if n == 0:
                pre_v[i] = prods[i]
            else:
                pre_v[i] += prods[i]
    all_passed(lambda copy: copy.wait_recv())
    last = [take(n) for n in (5, 6, 7)]
    squares = squares + last[0][0] + last[1][0] + last[2][0]
    sums = [pre_v[i] + (last[0][1][i] + last[1][1][i] + last[2][1][i]) for i in range(4)]
    lane = lax.broadcasted_iota(jnp.int32, (SEQ, 128), 1)
    scale = jnp.concatenate(
        [
            lax.rsqrt(
                jnp.sum(jnp.where(lane // F == p, squares, 0.0), axis=1, keepdims=True) / D + 1e-06
            )
            for p in range(PROPS)
        ],
        axis=0,
    )

    def pre(i):
        return (sums[i] * scale).astype(jnp.bfloat16).astype(jnp.float32)

    q_all = pre(0)
    q_all = q_all * sigmoid(q_all)
    f_all = fl + (1.0 - fl) * sigmoid(pre(1))
    k_all = 1.0 - f_all
    v_all = pre(2)

    def at(arr, t):
        return arr[t * SEQ : (t + 1) * SEQ]

    decay = None
    for t in range(PROPS):
        decay = at(f_all, t) if t == 0 else decay * at(f_all, t)
        scaled = at(q_all, t) * decay
        for h in range(2):
            a_v[h, pl.ds(4 * h + t, SEQ, stride=8), :] = scaled[:, h * HD : (h + 1) * HD]
    for s in range(SEQ):
        lhs = jnp.concatenate([a_v[0, 8 * s : 8 * s + 8], a_v[1, 8 * s : 8 * s + 8]], axis=1).astype(jnp.bfloat16)
        o_v[8 * s : 8 * s + 8] = jnp.dot(lhs, s0_v[s], preferred_element_type=jnp.float32)
    hg = small_v[:, D + 256 : D + 384]
    gate = pre(3)
    gate = gate * sigmoid(gate)
    for h in range(2):
        cols = slice(h * HD, (h + 1) * HD)
        for t in range(PROPS):
            weight = at(q_all, t)[:, cols]
            o = o_v[pl.ds(4 * h + t, SEQ, stride=8), :]
            for j in range(t, -1, -1):
                o = o + jnp.sum(weight * at(k_all, j)[:, cols], axis=1, keepdims=True) * at(v_all, j)[:, cols]
                if j:
                    weight = weight * at(f_all, j)[:, cols]
            norm = lax.rsqrt(jnp.mean(o * o, axis=1, keepdims=True) + 1e-05)
            mh_v[tp, h, t * SEQ : (t + 1) * SEQ, :] = (o * norm * hg * at(gate, t)[:, cols]).astype(jnp.bfloat16)
        for k in range(3):
            there = mh_v.at[tp, h]
            move(there, there, asem, bsem.at[(other(k) - tp + 3) % NTP], {"tp": other(k)}).start()

    def wait_gather(k):
        there = mh_v.at[(tp - k + NTP) % NTP]
        move(there, there, asem, bsem.at[k - 1], {"tp": tp}).wait_recv()

    wait_local(6)

    def piece(k, cols):
        place = (tp - k + NTP) % NTP
        w = wo_v[pl.ds(pl.multiple_of(place * 256, 256), 256), cols]
        return jnp.dot(jnp.concatenate([mh_v[place, 0], mh_v[place, 1]], axis=1), w, preferred_element_type=jnp.float32)

    for k in (0, 1, 3):
        if k:
            wait_gather(k)
        for n in range(4):
            cols = slice(n * 512, (n + 1) * 512)
            if k:
                acc_o[:, cols] += piece(k, cols)
            else:
                acc_o[:, cols] = piece(k, cols)
    wait_gather(2)

    def product(first, tiles):
        cols = pl.ds(pl.multiple_of(first * F, 128), tiles * 128)
        return acc_o[:, cols] + piece(2, cols)

    def blocks_of(out):
        found = []
        for q in range(out.shape[1] // 128):
            parts = [out[p * SEQ : (p + 1) * SEQ, q * 128 : (q + 1) * 128] for p in range(PROPS)]
            found += [part.astype(jnp.bfloat16) for part in swap_blocks(parts)]
        return found

    chunks = [(zt * 8 + 4 * q, 1) for zt, q in UNITS]
    outs = [product(*chunks[0]), product(*chunks[1])]
    ready = blocks_of(outs[0])
    for n, (first, _) in enumerate(chunks):
        if n + 2 < len(chunks):
            outs.append(product(*chunks[n + 2]))
        later = blocks_of(outs[n + 1]) if n + 1 < len(chunks) else None
        for j, block in enumerate(ready):
            tx2[first + j] = block
        zt, q = UNITS[n]
        slot = (z + 8 - zt) % 8
        reach = (slot * (8 - slot) + 1) // 8
        for k in range(4):
            d = first + (xc + k) % 4
            copy = move(tx2.at[d], rx2.at[slot, xc], ssem.at[1], osem.at[reach], {"kv": d})
            if k:
                copy.start()
            else:
                pl.when(d != kv)(copy.start)
        ready = later
    rx2[0, xc] = tx2[kv]

    for dist in ORDER:
        if dist in (0, 1, 3):
            group = (rx2.at[0, pl.ds(0, 7)], rx2.at[pl.ds(0, 4)], None, rx2.at[pl.ds(0, 3)])[dist]
            move(group, group, ssem.at[1], osem.at[(dist + 1) // 2], {"kv": kv}).wait_recv()
        mixed_ref[:, :, pl.ds(pl.multiple_of((z + dist) % 8 * 128, 128), 128)] = jnp.transpose(
            rx2[dist].reshape(128, 128)
        ).reshape(PROPS, F, 128)
    for side, count in ((0, 8 * len(DIRECT) - 1 + 6), (1, NKV - 1)):
        sent = (tx1, tx2)[side].at[pl.ds(0, count)]
        move(sent, sent, ssem.at[side], hsem.at[0], {"kv": kv}).wait_send()
    all_passed(lambda copy: copy.wait_send())
    sent = mh_v.at[pl.ds(0, 3)]
    move(sent, sent, asem, asem, {"tp": tp}).wait_send()


def tail(mixed_v, taken_v, mixed_hbm, taken_hbm, sem):
    for i in range(8):
        part = pl.ds(2 * i, 2)
        pltpu.make_async_copy(taken_v.at[part], taken_hbm.at[part], sem.at[0]).start()
    pltpu.make_async_copy(mixed_v, mixed_hbm, sem.at[1]).start()
    pltpu.make_async_copy(taken_v, taken_hbm, sem.at[0]).wait()
    pltpu.make_async_copy(mixed_v, mixed_hbm, sem.at[1]).wait()


def shards(hidden, norm_gain, w_query, w_forget, w_input, w_outgate, w_out, floor, head_gain, base_state, prev_forget, prev_input, accepted):
    any_spec = pl.BlockSpec(memory_space=pl.ANY)
    vmem = pl.BlockSpec(memory_space=pltpu.VMEM)
    bf, f32 = jnp.bfloat16, jnp.float32
    mixed, taken = pl.pallas_call(
        kernel,
        name="verify",
        out_shape=(
            pltpu.VMEM((PROPS, F, NKV * SEQ), bf),
            pltpu.VMEM((SEQ, 2, HD, HD), f32),
        ),
        in_specs=[any_spec] * 13,
        out_specs=(vmem, vmem),
        scratch_shapes=[
            pltpu.VMEM((PROPS, F, NKV * SEQ), bf),
            pltpu.VMEM((1, D + 384), f32),
            pltpu.VMEM((4, D, 256), bf),
            pltpu.VMEM((1024, D), bf),
            pltpu.VMEM((SEQ, 2, HD, HD), f32),
            pltpu.VMEM((2, SEQ, PROPS, 256), bf),
            pltpu.VMEM((1, SEQ), jnp.int32),
            pltpu.VMEM((SEQ, 2 * HD, HD), bf),
            pltpu.VMEM((NKV, SEQ, 128), bf),
            pltpu.VMEM((8, 8, SEQ, 128), bf),
            pltpu.VMEM((4, ROWS, 256), f32),
            pltpu.VMEM((2, 8 * SEQ, HD), f32),
            pltpu.VMEM((8 * SEQ, HD), f32),
            pltpu.VMEM((NTP, 2, ROWS, HD), bf),
            pltpu.VMEM((NKV, SEQ, 128), bf),
            pltpu.VMEM((8, 8, SEQ, 128), bf),
            pltpu.VMEM((ROWS, D), f32),
            pltpu.VMEM((3, 2, SEQ, 128), bf),
            pltpu.SemaphoreType.DMA((7,)),
            pltpu.SemaphoreType.DMA((2,)),
            pltpu.SemaphoreType.DMA((3,)),
            pltpu.SemaphoreType.DMA((2,)),
            pltpu.SemaphoreType.DMA,
            pltpu.SemaphoreType.DMA,
            pltpu.SemaphoreType.DMA((3,)),
            pltpu.SemaphoreType.DMA,
            pltpu.SemaphoreType.DMA((3,)),
        ],
        compiler_params=pltpu.CompilerParams(collective_id=0, has_side_effects=True),
    )(
        jnp.transpose(hidden, (1, 2, 0)),
        norm_gain.reshape(1, -1),
        w_query, w_forget, w_input, w_outgate, w_out,
        floor.reshape(1, -1),
        head_gain.reshape(1, -1),
        base_state, prev_forget, prev_input,
        accepted.reshape(1, -1),
    )
    mixed, taken = pl.pallas_call(
        tail,
        name="place",
        out_shape=(
            jax.ShapeDtypeStruct((PROPS, F, NKV * SEQ), bf),
            jax.ShapeDtypeStruct((SEQ, 2, HD, HD), f32),
        ),
        in_specs=[vmem] * 2,
        out_specs=(any_spec,) * 2,
        scratch_shapes=[pltpu.SemaphoreType.DMA((2,))],
    )(pltpu.with_memory_space_constraint(mixed, pltpu.VMEM), pltpu.with_memory_space_constraint(taken, pltpu.VMEM))
    return jnp.transpose(mixed, (2, 0, 1)), taken


def solution(mesh):
    in_specs = (
        P(None, None, "kv"), P(), P(None, "tp"), P(None, "tp"), P(None, "tp"), P(None, "tp"), P(), P("tp"), P(),
        P("kv", "tp", None, None), P("kv", None, "tp"), P("kv", None, "tp"), P("kv"),
    )
    out_specs = (P(None, None, "kv"), P("kv", "tp", None, None))
    return jax.shard_map(shards, mesh=mesh, in_specs=in_specs, out_specs=out_specs, check_vma=False)
```

```python
import functools

import jax
import jax.numpy as jnp
from jax import lax
from jax.experimental import pallas as pl
from jax.experimental.pallas import tpu as pltpu
from jax.sharding import PartitionSpec as P

D = 2048
HD = 128
PROPS = 4
NKV = 64
NTP = 4
SEQ = 16
ROWS = SEQ * PROPS
F = D // NKV
EARLY = 4
MESH = pl.DeviceIdType.MESH
ORDER = (0, 1, 7, 2, 6, 3, 5, 4)
RELAYED = (4, 3, 5)
DIRECT = (2, 6, 1, 7, 0)
UNITS = tuple(sorted(((zt, q) for zt in range(8) for q in range(2)), key=lambda u: (min(u[0], 4) + 1.2 * u[1], u)))
HOLD = {3: 0, 5: 1, 4: 2}


def swap_blocks(parts):
    lane = lax.broadcasted_iota(jnp.int32, parts[0].shape, parts[0].ndim - 1)
    axis = parts[0].ndim - 1
    place = lane // 32
    found = []
    for i in range(4):
        block = parts[i]
        for r in range(1, 4):
            block = jnp.where(place == (i + r) % 4, pltpu.roll(parts[(i + r) % 4], 32 * r, axis), block)
        found.append(block)
    return found


def sigmoid(x):
    return jax.nn.sigmoid(x)


def kernel(
    x_hbm, gain_hbm, wq_hbm, wf_hbm, wi_hbm, wg_hbm, wo_hbm, floor_hbm, hgain_hbm,
    base_hbm, pf_hbm, pv_hbm, acc_hbm,
    mixed_ref, taken_ref,
    x_v, small_v, w_v, wo_v, base_v, pfv_v, acc_v,
    s0_v, tx1, rx1, pre_v, a_v, o_v, mh_v, tx2, rx2,
    acc_o,
    hold,
    lsem, ssem, rsem, hsem, fsem, gsem, osem, asem, bsem,
):
    kv = lax.axis_index("kv")
    tp = lax.axis_index("tp")
    z = kv // 8
    xc = kv % 8
    mine = xc % 2
    xr_base = xc // 2
    turn = [(tp + 2 * mine + part) % 4 for part in range(2)]
    xd = [(xr_base + 4 - turn[part]) % 4 for part in range(2)]

    barrier = pltpu.get_barrier_semaphore()
    def local(src, dst, n):
        return pltpu.make_async_copy(src, dst, lsem.at[n])

    small = ((gain_hbm, 0, D), (floor_hbm, D, 256), (hgain_hbm, D + 256, HD))
    locals_ = [
        local(x_hbm, x_v, 0),
        local(pf_hbm, pfv_v.at[0], 1),
        local(pv_hbm, pfv_v.at[1], 1),
        local(acc_hbm, acc_v, 2),
        *(local(ref, small_v.at[:, pl.ds(at, n)], 3) for ref, at, n in small),
        local(base_hbm, base_v, 4),
        *(local(ref, w_v.at[i], 5) for i, ref in enumerate((wq_hbm, wf_hbm, wi_hbm, wg_hbm))),
        local(wo_hbm, wo_v, 6),
    ]
    whole = [x_v, pfv_v, acc_v, small_v, base_v, w_v, wo_v]

    def wait_local(n):
        local(whole[n], whole[n], n).wait()

    locals_[0].start()


    def greet(where):
        pl.semaphore_signal(barrier, inc=1, device_id=where, device_id_type=MESH)

    for dist in RELAYED:
        greet({"kv": (z + dist) % 8 * 8 + xc})
    for part in range(2):
        for r in (2, 1, 3, 0):
            for m in range(2):
                core = (mine + m) % 2
                where = {"kv": z * 8 + (xr_base + r) % 4 * 2 + core, "tp": (r + 2 * core + 4 - part) % 4}
                if r == 0 and m == 0:
                    pl.when(turn[part] != 0)(functools.partial(greet, where))
                else:
                    greet(where)
    for dist in DIRECT:
        for k in range(1 if dist == 0 else 0, 8):
            greet({"kv": (z + dist) % 8 * 8 + (xc + 4 + k) % 8 if dist else z * 8 + (xc + k) % 8})
    for k in range(1, NTP):
        greet({"tp": (tp + k) % NTP})

    for copy in locals_[1:]:
        copy.start()

    wait_local(0)
    for b in range(8):
        block = x_v[:, :, 128 * b : 128 * (b + 1)].reshape(128, 128)
        tx1[8 * b : 8 * (b + 1)] = jnp.transpose(block).reshape(8, SEQ, 128)

    for n in range(1, 5):
        wait_local(n)
    fl = small_v[:, D : D + 256]
    row4 = lax.broadcasted_iota(jnp.int32, (PROPS, 2 * HD), 0)
    a_v[...] = jnp.zeros_like(a_v)
    ones_row = (lax.broadcasted_iota(jnp.int32, (8, HD), 0) == 4).astype(jnp.float32)
    seq_lane = lax.broadcasted_iota(jnp.int32, (1, SEQ), 1)

    def state_step(s, c):
        count = jnp.sum(jnp.where(seq_lane == s, acc_v[...], 0), axis=1, keepdims=True)
        live = row4 < count
        f = fl + (1.0 - fl) * sigmoid(pfv_v[0, s].astype(jnp.float32))
        k = jnp.where(live, 1.0 - f, 0.0)
        f = jnp.where(live, f, 1.0)
        v = pfv_v[1, s].astype(jnp.float32)
        f0, f1, f2, f3 = (f[j : j + 1] for j in range(4))
        f23 = f2 * f3
        f123 = f1 * f23
        coef = jnp.concatenate(
            [k[0:1] * f123, k[1:2] * f23, k[2:3] * f3, k[3:4], f0 * f123, jnp.zeros((3, 2 * HD), jnp.float32)],
            axis=0,
        )
        high = coef.astype(jnp.bfloat16).astype(jnp.float32)
        rest = coef - high
        mid = rest.astype(jnp.bfloat16).astype(jnp.float32)
        lhs = jnp.concatenate([high, mid, rest - mid, jnp.zeros((8, 2 * HD), jnp.float32)], axis=0).astype(jnp.bfloat16)
        for h in range(2):
            cols = slice(h * HD, (h + 1) * HD)
            rows = jnp.concatenate([v[:, cols], jnp.zeros((4, HD), jnp.float32)], axis=0)
            rows = jnp.concatenate([ones_row, rows], axis=1)
            rhs = jnp.concatenate([rows] * 4, axis=0).astype(jnp.bfloat16)
            spread = lax.dot_general(
                lhs[:, cols], rhs, (((0,), (0,)), ((), ())), preferred_element_type=jnp.float32
            )
            new = spread[:, :HD] * base_v[s, h] + spread[:, HD:]
            taken_ref[s, h] = new
            s0_v[s, cols, :] = new.astype(jnp.bfloat16)
        return c

    lax.fori_loop(0, EARLY, state_step, 0, unroll=4)

    others = (turn[0] + 3) // 4 + (turn[1] + 3) // 4
    pl.semaphore_wait(barrier, 8 * len(DIRECT) - 1 + len(RELAYED) + NTP - 1 + 14 + others)


    def move(src, dst, send_sem, recv_sem, where):
        return pltpu.make_async_remote_copy(
            src_ref=src, dst_ref=dst, send_sem=send_sem, recv_sem=recv_sem, device_id=where, device_id_type=MESH
        )

    def send_relayed(dist):
        zd = (z + dist) % 8
        slot = HOLD[8 - dist]
        move(
            tx1.at[pl.ds(zd * 8 + xd[slot // 2] * 2, 2)], hold.at[slot], ssem.at[0], hsem.at[slot // 2],
            {"kv": zd * 8 + xc},
        ).start()

    def send_direct(side, dist):
        tx, rx = ((tx1, rx1), (tx2, rx2))[side]
        zd = (z + dist) % 8
        slot = ORDER.index((8 - dist) % 8)
        for k in range(1 if dist == 0 else 0, 8):
            d = zd * 8 + (xc + k) % 8
            move(tx.at[d], rx.at[slot, xc], ssem.at[side], rsem.at[(slot + 1) // 2], {"kv": d}).start()

    def other(k):
        return tp if k == 3 else k + (k - tp + 4) // 4

    def pass_on(part):
        held = hold.at[pl.ds(2 * part, 2 - part)]
        to = rx1.at[pl.ds(5 + 2 * part, 2 - part)]
        move(held, held, ssem.at[0], hsem.at[part], {"kv": kv}).wait_recv()
        for m in range(2):
            core = (mine + m) % 2
            for k in range(NTP):
                copy = move(
                    held.at[:, core], to.at[:, xc], fsem, gsem,
                    {"kv": z * 8 + xd[part] * 2 + core, "tp": other(k)},
                )
                if m == 0 and k == 3:
                    pl.when(turn[part] != 0)(copy.start)

                    @pl.when(turn[part] == 0)
                    def _():
                        for b in range(2 - part):
                            rx1[5 + 2 * part + b, xc] = hold[2 * part + b, core]
                else:
                    copy.start()

    def all_passed(wait):
        for when, blocks in ((turn[0] == 0, 22), (turn[1] == 0, 23), (turn[0] * turn[1] != 0, 24)):
            some = tx1.at[pl.ds(0, blocks)]
            pl.when(when)(functools.partial(wait, move(some, some, fsem, gsem, {"kv": kv})))

    def wait_direct(part):
        group = rx1.at[pl.ds(1, 2)] if part else rx1.at[0, pl.ds(0, 7)]
        move(group, group, ssem.at[0], rsem.at[part], {"kv": kv}).wait_recv()

    for dist in RELAYED:
        send_relayed(dist)
    rx1[0, xc] = tx1[kv]

    lax.fori_loop(EARLY, SEQ, state_step, 0, unroll=4)
    for dist in DIRECT:
        send_direct(0, dist)
    pass_on(0)
    pass_on(1)
    wait_local(5)
    squares = jnp.zeros((SEQ, 128), jnp.float32)

    def take(n):
        zs = (z + ORDER[n]) % 8
        vals = rx1[n].astype(jnp.float32)
        tiles = []
        for q in range(2):
            swapped = swap_blocks([vals[4 * q + i] for i in range(4)])
            gain = small_v[:, pl.ds(pl.multiple_of(zs * 256 + q * 128, 128), 128)]
            tiles.append(jnp.concatenate([(part * gain).astype(jnp.bfloat16) for part in swapped], axis=0))
        lhs = jnp.concatenate(tiles, axis=1)
        prods = [
            jnp.dot(lhs, w_v[i, pl.ds(pl.multiple_of(zs * 256, 256), 256), :], preferred_element_type=jnp.float32)
            for i in range(4)
        ]
        return jnp.sum(vals * vals, axis=0), prods

    for n in range(5):
        if n in (0, 1, 3):
            wait_direct((n + 1) // 2)
        part, prods = take(n)
        squares = squares + part
        for i in range(4):
            if n == 0:
                pre_v[i] = prods[i]
            else:
                pre_v[i] += prods[i]
    all_passed(lambda copy: copy.wait_recv())
    last = [take(n) for n in (5, 6, 7)]
    squares = squares + last[0][0] + last[1][0] + last[2][0]
    sums = [pre_v[i] + (last[0][1][i] + last[1][1][i] + last[2][1][i]) for i in range(4)]
    lane = lax.broadcasted_iota(jnp.int32, (SEQ, 128), 1)
    scale = jnp.concatenate(
        [
            lax.rsqrt(
                jnp.sum(jnp.where(lane // F == p, squares, 0.0), axis=1, keepdims=True) / D + 1e-06
            )
            for p in range(PROPS)
        ],
        axis=0,
    )

    def pre(i):
        return (sums[i] * scale).astype(jnp.bfloat16).astype(jnp.float32)

    q_all = pre(0)
    q_all = q_all * sigmoid(q_all)
    f_all = fl + (1.0 - fl) * sigmoid(pre(1))
    k_all = 1.0 - f_all
    v_all = pre(2)

    def at(arr, t):
        return arr[t * SEQ : (t + 1) * SEQ]

    decay = None
    for t in range(PROPS):
        decay = at(f_all, t) if t == 0 else decay * at(f_all, t)
        scaled = at(q_all, t) * decay
        for h in range(2):
            a_v[h, pl.ds(4 * h + t, SEQ, stride=8), :] = scaled[:, h * HD : (h + 1) * HD]
    for s in range(SEQ):
        lhs = jnp.concatenate([a_v[0, 8 * s : 8 * s + 8], a_v[1, 8 * s : 8 * s + 8]], axis=1).astype(jnp.bfloat16)
        o_v[8 * s : 8 * s + 8] = jnp.dot(lhs, s0_v[s], preferred_element_type=jnp.float32)
    hg = small_v[:, D + 256 : D + 384]
    gate = pre(3)
    gate = gate * sigmoid(gate)
    for h in range(2):
        cols = slice(h * HD, (h + 1) * HD)
        for t in range(PROPS):
            weight = at(q_all, t)[:, cols]
            o = o_v[pl.ds(4 * h + t, SEQ, stride=8), :]
            for j in range(t, -1, -1):
                o = o + jnp.sum(weight * at(k_all, j)[:, cols], axis=1, keepdims=True) * at(v_all, j)[:, cols]
                if j:
                    weight = weight * at(f_all, j)[:, cols]
            norm = lax.rsqrt(jnp.mean(o * o, axis=1, keepdims=True) + 1e-05)
            mh_v[tp, h, t * SEQ : (t + 1) * SEQ, :] = (o * norm * hg * at(gate, t)[:, cols]).astype(jnp.bfloat16)
        for k in range(3):
            there = mh_v.at[tp, h]
            move(there, there, asem, bsem.at[(other(k) - tp + 3) % NTP], {"tp": other(k)}).start()

    def wait_gather(k):
        there = mh_v.at[(tp - k + NTP) % NTP]
        move(there, there, asem, bsem.at[k - 1], {"tp": tp}).wait_recv()

    wait_local(6)

    def piece(k, cols):
        place = (tp - k + NTP) % NTP
        w = wo_v[pl.ds(pl.multiple_of(place * 256, 256), 256), cols]
        return jnp.dot(jnp.concatenate([mh_v[place, 0], mh_v[place, 1]], axis=1), w, preferred_element_type=jnp.float32)

    for k in (0, 1, 3):
        if k:
            wait_gather(k)
        for n in range(4):
            cols = slice(n * 512, (n + 1) * 512)
            if k:
                acc_o[:, cols] += piece(k, cols)
            else:
                acc_o[:, cols] = piece(k, cols)
    wait_gather(2)

    def product(first, tiles):
        cols = pl.ds(pl.multiple_of(first * F, 128), tiles * 128)
        return acc_o[:, cols] + piece(2, cols)

    def blocks_of(out):
        found = []
        for q in range(out.shape[1] // 128):
            parts = [out[p * SEQ : (p + 1) * SEQ, q * 128 : (q + 1) * 128] for p in range(PROPS)]
            found += [part.astype(jnp.bfloat16) for part in swap_blocks(parts)]
        return found

    chunks = [(zt * 8 + 4 * q, 1) for zt, q in UNITS]
    outs = [product(*chunks[0]), product(*chunks[1])]
    ready = blocks_of(outs[0])
    for n, (first, _) in enumerate(chunks):
        if n + 2 < len(chunks):
            outs.append(product(*chunks[n + 2]))
        later = blocks_of(outs[n + 1]) if n + 1 < len(chunks) else None
        for j, block in enumerate(ready):
            tx2[first + j] = block
        zt, q = UNITS[n]
        slot = (z + 8 - zt) % 8
        reach = (slot * (8 - slot) + 1) // 8
        for k in range(4):
            d = first + (xc + k) % 4
            copy = move(tx2.at[d], rx2.at[slot, xc], ssem.at[1], osem.at[reach], {"kv": d})
            if k:
                copy.start()
            else:
                pl.when(d != kv)(copy.start)
        ready = later
    rx2[0, xc] = tx2[kv]

    for dist in ORDER:
        if dist in (0, 1, 3):
            group = (rx2.at[0, pl.ds(0, 7)], rx2.at[pl.ds(0, 4)], None, rx2.at[pl.ds(0, 3)])[dist]
            move(group, group, ssem.at[1], osem.at[(dist + 1) // 2], {"kv": kv}).wait_recv()
        mixed_ref[:, :, pl.ds(pl.multiple_of((z + dist) % 8 * 128, 128), 128)] = jnp.transpose(
            rx2[dist].reshape(128, 128)
        ).reshape(PROPS, F, 128)
    for side, count in ((0, 8 * len(DIRECT) - 1 + 6), (1, NKV - 1)):
        sent = (tx1, tx2)[side].at[pl.ds(0, count)]
        move(sent, sent, ssem.at[side], hsem.at[0], {"kv": kv}).wait_send()
    all_passed(lambda copy: copy.wait_send())
    sent = mh_v.at[pl.ds(0, 3)]
    move(sent, sent, asem, asem, {"tp": tp}).wait_send()


def tail(mixed_v, taken_v, mixed_hbm, taken_hbm, sem):
    for i in range(8):
        part = pl.ds(2 * i, 2)
        pltpu.make_async_copy(taken_v.at[part], taken_hbm.at[part], sem.at[0]).start()
    pltpu.make_async_copy(mixed_v, mixed_hbm, sem.at[1]).start()
    pltpu.make_async_copy(taken_v, taken_hbm, sem.at[0]).wait()
    pltpu.make_async_copy(mixed_v, mixed_hbm, sem.at[1]).wait()


def shards(hidden, norm_gain, w_query, w_forget, w_input, w_outgate, w_out, floor, head_gain, base_state, prev_forget, prev_input, accepted):
    any_spec = pl.BlockSpec(memory_space=pl.ANY)
    vmem = pl.BlockSpec(memory_space=pltpu.VMEM)
    bf, f32 = jnp.bfloat16, jnp.float32
    mixed, taken = pl.pallas_call(
        kernel,
        name="verify",
        out_shape=(
            pltpu.VMEM((PROPS, F, NKV * SEQ), bf),
            pltpu.VMEM((SEQ, 2, HD, HD), f32),
        ),
        in_specs=[any_spec] * 13,
        out_specs=(vmem, vmem),
        scratch_shapes=[
            pltpu.VMEM((PROPS, F, NKV * SEQ), bf),
            pltpu.VMEM((1, D + 384), f32),
            pltpu.VMEM((4, D, 256), bf),
            pltpu.VMEM((1024, D), bf),
            pltpu.VMEM((SEQ, 2, HD, HD), f32),
            pltpu.VMEM((2, SEQ, PROPS, 256), bf),
            pltpu.VMEM((1, SEQ), jnp.int32),
            pltpu.VMEM((SEQ, 2 * HD, HD), bf),
            pltpu.VMEM((NKV, SEQ, 128), bf),
            pltpu.VMEM((8, 8, SEQ, 128), bf),
            pltpu.VMEM((4, ROWS, 256), f32),
            pltpu.VMEM((2, 8 * SEQ, HD), f32),
            pltpu.VMEM((8 * SEQ, HD), f32),
            pltpu.VMEM((NTP, 2, ROWS, HD), bf),
            pltpu.VMEM((NKV, SEQ, 128), bf),
            pltpu.VMEM((8, 8, SEQ, 128), bf),
            pltpu.VMEM((ROWS, D), f32),
            pltpu.VMEM((3, 2, SEQ, 128), bf),
            pltpu.SemaphoreType.DMA((7,)),
            pltpu.SemaphoreType.DMA((2,)),
            pltpu.SemaphoreType.DMA((3,)),
            pltpu.SemaphoreType.DMA((2,)),
            pltpu.SemaphoreType.DMA,
            pltpu.SemaphoreType.DMA,
            pltpu.SemaphoreType.DMA((3,)),
            pltpu.SemaphoreType.DMA,
            pltpu.SemaphoreType.DMA((3,)),
        ],
        compiler_params=pltpu.CompilerParams(collective_id=0, has_side_effects=True),
    )(
        jnp.transpose(hidden, (1, 2, 0)),
        norm_gain.reshape(1, -1),
        w_query, w_forget, w_input, w_outgate, w_out,
        floor.reshape(1, -1),
        head_gain.reshape(1, -1),
        base_state, prev_forget, prev_input,
        accepted.reshape(1, -1),
    )
    mixed, taken = pl.pallas_call(
        tail,
        name="place",
        out_shape=(
            jax.ShapeDtypeStruct((PROPS, F, NKV * SEQ), bf),
            jax.ShapeDtypeStruct((SEQ, 2, HD, HD), f32),
        ),
        in_specs=[vmem] * 2,
        out_specs=(any_spec,) * 2,
        scratch_shapes=[pltpu.SemaphoreType.DMA((2,))],
    )(pltpu.with_memory_space_constraint(mixed, pltpu.VMEM), pltpu.with_memory_space_constraint(taken, pltpu.VMEM))
    return jnp.transpose(mixed, (2, 0, 1)), taken


def solution(mesh):
    in_specs = (
        P(None, None, "kv"), P(), P(None, "tp"), P(None, "tp"), P(None, "tp"), P(None, "tp"), P(), P("tp"), P(),
        P("kv", "tp", None, None), P("kv", None, "tp"), P("kv", None, "tp"), P("kv"),
    )
    out_specs = (P(None, None, "kv"), P("kv", "tp", None, None))
    return jax.shard_map(shards, mesh=mesh, in_specs=in_specs, out_specs=out_specs, check_vma=False)
```

```python
import functools

import jax
import jax.numpy as jnp
from jax import lax
from jax.experimental import pallas as pl
from jax.experimental.pallas import tpu as pltpu
from jax.sharding import PartitionSpec as P

D = 2048
HD = 128
PROPS = 4
NKV = 64
NTP = 4
SEQ = 16
ROWS = SEQ * PROPS
F = D // NKV
EARLY = 4
MESH = pl.DeviceIdType.MESH
ORDER = (0, 1, 7, 2, 6, 3, 5, 4)
RELAYED = (4, 3, 5)
DIRECT = (2, 6, 1, 7, 0)
UNITS = tuple(sorted(((zt, q) for zt in range(8) for q in range(2)), key=lambda u: (min(u[0], 4) + 1.2 * u[1], u)))
HOLD = {3: 0, 5: 1, 4: 2}


def swap_blocks(parts):
    lane = lax.broadcasted_iota(jnp.int32, parts[0].shape, parts[0].ndim - 1)
    axis = parts[0].ndim - 1
    place = lane // 32
    found = []
    for i in range(4):
        block = parts[i]
        for r in range(1, 4):
            block = jnp.where(place == (i + r) % 4, pltpu.roll(parts[(i + r) % 4], 32 * r, axis), block)
        found.append(block)
    return found


def sigmoid(x):
    return jax.nn.sigmoid(x)


def kernel(
    x_hbm, gain_hbm, wq_hbm, wf_hbm, wi_hbm, wg_hbm, wo_hbm, floor_hbm, hgain_hbm,
    base_hbm, pf_hbm, pv_hbm, acc_hbm,
    mixed_ref, taken_ref,
    x_v, small_v, w_v, wo_v, base_v, pfv_v, acc_v,
    s0_v, tx1, rx1, pre_v, a_v, o_v, mh_v, tx2, rx2,
    acc_o,
    hold,
    lsem, ssem, rsem, hsem, fsem, gsem, osem, asem, bsem,
):
    kv = lax.axis_index("kv")
    tp = lax.axis_index("tp")
    z = kv // 8
    xc = kv % 8
    mine = xc % 2
    xr_base = xc // 2
    turn = [(1 * tp + 2 * mine + 2 * part + 1) % 4 for part in range(2)]
    xd = [(xr_base + 4 - turn[part]) % 4 for part in range(2)]

    barrier = pltpu.get_barrier_semaphore()
    def local(src, dst, n):
        return pltpu.make_async_copy(src, dst, lsem.at[n])

    small = ((gain_hbm, 0, D), (floor_hbm, D, 256), (hgain_hbm, D + 256, HD))
    locals_ = [
        local(x_hbm, x_v, 0),
        local(pf_hbm, pfv_v.at[0], 1),
        local(pv_hbm, pfv_v.at[1], 1),
        local(acc_hbm, acc_v, 2),
        *(local(ref, small_v.at[:, pl.ds(at, n)], 3) for ref, at, n in small),
        local(base_hbm, base_v, 4),
        *(local(ref, w_v.at[i], 5) for i, ref in enumerate((wq_hbm, wf_hbm, wi_hbm, wg_hbm))),
        local(wo_hbm, wo_v, 6),
    ]
    whole = [x_v, pfv_v, acc_v, small_v, base_v, w_v, wo_v]

    def wait_local(n):
        local(whole[n], whole[n], n).wait()

    locals_[0].start()


    def greet(where):
        pl.semaphore_signal(barrier, inc=1, device_id=where, device_id_type=MESH)

    for dist in RELAYED:
        greet({"kv": (z + dist) % 8 * 8 + xc})
    for part in range(2):
        for r in (2, 1, 3, 0):
            for m in range(2):
                core = (mine + m) % 2
                where = {"kv": z * 8 + (xr_base + r) % 4 * 2 + core, "tp": 1 * (r + 2 * core + 2 * part + 3) % 4}
                if r == 0 and m == 0:
                    pl.when(turn[part] != 0)(functools.partial(greet, where))
                else:
                    greet(where)
    for dist in DIRECT:
        for k in range(1 if dist == 0 else 0, 8):
            greet({"kv": (z + dist) % 8 * 8 + (xc + 4 + k) % 8 if dist else z * 8 + (xc + k) % 8})
    for k in range(1, NTP):
        greet({"tp": (tp + k) % NTP})

    for copy in locals_[1:]:
        copy.start()

    wait_local(0)
    for b in range(8):
        block = x_v[:, :, 128 * b : 128 * (b + 1)].reshape(128, 128)
        tx1[8 * b : 8 * (b + 1)] = jnp.transpose(block).reshape(8, SEQ, 128)

    for n in range(1, 5):
        wait_local(n)
    fl = small_v[:, D : D + 256]
    row4 = lax.broadcasted_iota(jnp.int32, (PROPS, 2 * HD), 0)
    a_v[...] = jnp.zeros_like(a_v)
    ones_row = (lax.broadcasted_iota(jnp.int32, (8, HD), 0) == 4).astype(jnp.float32)
    seq_lane = lax.broadcasted_iota(jnp.int32, (1, SEQ), 1)

    def state_step(s, c):
        count = jnp.sum(jnp.where(seq_lane == s, acc_v[...], 0), axis=1, keepdims=True)
        live = row4 < count
        f = fl + (1.0 - fl) * sigmoid(pfv_v[0, s].astype(jnp.float32))
        k = jnp.where(live, 1.0 - f, 0.0)
        f = jnp.where(live, f, 1.0)
        v = pfv_v[1, s].astype(jnp.float32)
        f0, f1, f2, f3 = (f[j : j + 1] for j in range(4))
        f23 = f2 * f3
        f123 = f1 * f23
        coef = jnp.concatenate(
            [k[0:1] * f123, k[1:2] * f23, k[2:3] * f3, k[3:4], f0 * f123, jnp.zeros((3, 2 * HD), jnp.float32)],
            axis=0,
        )
        high = coef.astype(jnp.bfloat16).astype(jnp.float32)
        rest = coef - high
        mid = rest.astype(jnp.bfloat16).astype(jnp.float32)
        lhs = jnp.concatenate([high, mid, rest - mid, jnp.zeros((8, 2 * HD), jnp.float32)], axis=0).astype(jnp.bfloat16)
        for h in range(2):
            cols = slice(h * HD, (h + 1) * HD)
            rows = jnp.concatenate([v[:, cols], jnp.zeros((4, HD), jnp.float32)], axis=0)
            rows = jnp.concatenate([ones_row, rows], axis=1)
            rhs = jnp.concatenate([rows] * 4, axis=0).astype(jnp.bfloat16)
            spread = lax.dot_general(
                lhs[:, cols], rhs, (((0,), (0,)), ((), ())), preferred_element_type=jnp.float32
            )
            new = spread[:, :HD] * base_v[s, h] + spread[:, HD:]
            taken_ref[s, h] = new
            s0_v[s, cols, :] = new.astype(jnp.bfloat16)
        return c

    lax.fori_loop(0, EARLY, state_step, 0, unroll=4)

    others = (turn[0] + 3) // 4 + (turn[1] + 3) // 4
    pl.semaphore_wait(barrier, 8 * len(DIRECT) - 1 + len(RELAYED) + NTP - 1 + 14 + others)


    def move(src, dst, send_sem, recv_sem, where):
        return pltpu.make_async_remote_copy(
            src_ref=src, dst_ref=dst, send_sem=send_sem, recv_sem=recv_sem, device_id=where, device_id_type=MESH
        )

    def send_relayed(dist):
        zd = (z + dist) % 8
        slot = HOLD[8 - dist]
        move(
            tx1.at[pl.ds(zd * 8 + xd[slot // 2] * 2, 2)], hold.at[slot], ssem.at[0], hsem.at[slot // 2],
            {"kv": zd * 8 + xc},
        ).start()

    def send_direct(side, dist):
        tx, rx = ((tx1, rx1), (tx2, rx2))[side]
        zd = (z + dist) % 8
        slot = ORDER.index((8 - dist) % 8)
        for k in range(1 if dist == 0 else 0, 8):
            d = zd * 8 + (xc + k) % 8
            move(tx.at[d], rx.at[slot, xc], ssem.at[side], rsem.at[(slot + 1) // 2], {"kv": d}).start()

    def other(k):
        return tp if k == 3 else k + (k - tp + 4) // 4

    def pass_on(part):
        held = hold.at[pl.ds(2 * part, 2 - part)]
        to = rx1.at[pl.ds(5 + 2 * part, 2 - part)]
        move(held, held, ssem.at[0], hsem.at[part], {"kv": kv}).wait_recv()
        for m in range(2):
            core = (mine + m) % 2
            for k in range(NTP):
                copy = move(
                    held.at[:, core], to.at[:, xc], fsem, gsem,
                    {"kv": z * 8 + xd[part] * 2 + core, "tp": other(k)},
                )
                if m == 0 and k == 3:
                    pl.when(turn[part] != 0)(copy.start)

                    @pl.when(turn[part] == 0)
                    def _():
                        for b in range(2 - part):
                            rx1[5 + 2 * part + b, xc] = hold[2 * part + b, core]
                else:
                    copy.start()

    def all_passed(wait):
        for when, blocks in ((turn[0] == 0, 22), (turn[1] == 0, 23), (turn[0] * turn[1] != 0, 24)):
            some = tx1.at[pl.ds(0, blocks)]
            pl.when(when)(functools.partial(wait, move(some, some, fsem, gsem, {"kv": kv})))

    def wait_direct(part):
        group = rx1.at[pl.ds(1, 2)] if part else rx1.at[0, pl.ds(0, 7)]
        move(group, group, ssem.at[0], rsem.at[part], {"kv": kv}).wait_recv()

    for dist in RELAYED:
        send_relayed(dist)
    rx1[0, xc] = tx1[kv]

    lax.fori_loop(EARLY, SEQ, state_step, 0, unroll=4)
    for dist in DIRECT:
        send_direct(0, dist)
    pass_on(0)
    pass_on(1)
    wait_local(5)
    squares = jnp.zeros((SEQ, 128), jnp.float32)

    def take(n):
        zs = (z + ORDER[n]) % 8
        vals = rx1[n].astype(jnp.float32)
        tiles = []
        for q in range(2):
            swapped = swap_blocks([vals[4 * q + i] for i in range(4)])
            gain = small_v[:, pl.ds(pl.multiple_of(zs * 256 + q * 128, 128), 128)]
            tiles.append(jnp.concatenate([(part * gain).astype(jnp.bfloat16) for part in swapped], axis=0))
        lhs = jnp.concatenate(tiles, axis=1)
        prods = [
            jnp.dot(lhs, w_v[i, pl.ds(pl.multiple_of(zs * 256, 256), 256), :], preferred_element_type=jnp.float32)
            for i in range(4)
        ]
        return jnp.sum(vals * vals, axis=0), prods

    for n in range(5):
        if n in (0, 1, 3):
            wait_direct((n + 1) // 2)
        part, prods = take(n)
        squares = squares + part
        for i in range(4):
            if n == 0:
                pre_v[i] = prods[i]
            else:
                pre_v[i] += prods[i]
    all_passed(lambda copy: copy.wait_recv())
    last = [take(n) for n in (5, 6, 7)]
    squares = squares + last[0][0] + last[1][0] + last[2][0]
    sums = [pre_v[i] + (last[0][1][i] + last[1][1][i] + last[2][1][i]) for i in range(4)]
    lane = lax.broadcasted_iota(jnp.int32, (SEQ, 128), 1)
    scale = jnp.concatenate(
        [
            lax.rsqrt(
                jnp.sum(jnp.where(lane // F == p, squares, 0.0), axis=1, keepdims=True) / D + 1e-06
            )
            for p in range(PROPS)
        ],
        axis=0,
    )

    def pre(i):
        return (sums[i] * scale).astype(jnp.bfloat16).astype(jnp.float32)

    q_all = pre(0)
    q_all = q_all * sigmoid(q_all)
    f_all = fl + (1.0 - fl) * sigmoid(pre(1))
    k_all = 1.0 - f_all
    v_all = pre(2)

    def at(arr, t):
        return arr[t * SEQ : (t + 1) * SEQ]

    decay = None
    for t in range(PROPS):
        decay = at(f_all, t) if t == 0 else decay * at(f_all, t)
        scaled = at(q_all, t) * decay
        for h in range(2):
            a_v[h, pl.ds(4 * h + t, SEQ, stride=8), :] = scaled[:, h * HD : (h + 1) * HD]
    for s in range(SEQ):
        lhs = jnp.concatenate([a_v[0, 8 * s : 8 * s + 8], a_v[1, 8 * s : 8 * s + 8]], axis=1).astype(jnp.bfloat16)
        o_v[8 * s : 8 * s + 8] = jnp.dot(lhs, s0_v[s], preferred_element_type=jnp.float32)
    hg = small_v[:, D + 256 : D + 384]
    gate = pre(3)
    gate = gate * sigmoid(gate)
    for h in range(2):
        cols = slice(h * HD, (h + 1) * HD)
        for t in range(PROPS):
            weight = at(q_all, t)[:, cols]
            o = o_v[pl.ds(4 * h + t, SEQ, stride=8), :]
            for j in range(t, -1, -1):
                o = o + jnp.sum(weight * at(k_all, j)[:, cols], axis=1, keepdims=True) * at(v_all, j)[:, cols]
                if j:
                    weight = weight * at(f_all, j)[:, cols]
            norm = lax.rsqrt(jnp.mean(o * o, axis=1, keepdims=True) + 1e-05)
            mh_v[tp, h, t * SEQ : (t + 1) * SEQ, :] = (o * norm * hg * at(gate, t)[:, cols]).astype(jnp.bfloat16)
        for k in range(3):
            there = mh_v.at[tp, h]
            move(there, there, asem, bsem.at[(other(k) - tp + 3) % NTP], {"tp": other(k)}).start()

    def wait_gather(k):
        there = mh_v.at[(tp - k + NTP) % NTP]
        move(there, there, asem, bsem.at[k - 1], {"tp": tp}).wait_recv()

    wait_local(6)

    def piece(k, cols):
        place = (tp - k + NTP) % NTP
        w = wo_v[pl.ds(pl.multiple_of(place * 256, 256), 256), cols]
        return jnp.dot(jnp.concatenate([mh_v[place, 0], mh_v[place, 1]], axis=1), w, preferred_element_type=jnp.float32)

    for k in (0, 1, 3):
        if k:
            wait_gather(k)
        for n in range(4):
            cols = slice(n * 512, (n + 1) * 512)
            if k:
                acc_o[:, cols] += piece(k, cols)
            else:
                acc_o[:, cols] = piece(k, cols)
    wait_gather(2)

    def product(first, tiles):
        cols = pl.ds(pl.multiple_of(first * F, 128), tiles * 128)
        return acc_o[:, cols] + piece(2, cols)

    def blocks_of(out):
        found = []
        for q in range(out.shape[1] // 128):
            parts = [out[p * SEQ : (p + 1) * SEQ, q * 128 : (q + 1) * 128] for p in range(PROPS)]
            found += [part.astype(jnp.bfloat16) for part in swap_blocks(parts)]
        return found

    chunks = [(zt * 8 + 4 * q, 1) for zt, q in UNITS]
    outs = [product(*chunks[0]), product(*chunks[1])]
    ready = blocks_of(outs[0])
    for n, (first, _) in enumerate(chunks):
        if n + 2 < len(chunks):
            outs.append(product(*chunks[n + 2]))
        later = blocks_of(outs[n + 1]) if n + 1 < len(chunks) else None
        for j, block in enumerate(ready):
            tx2[first + j] = block
        zt, q = UNITS[n]
        slot = (z + 8 - zt) % 8
        reach = (slot * (8 - slot) + 1) // 8
        for k in range(4):
            d = first + (xc + k) % 4
            copy = move(tx2.at[d], rx2.at[slot, xc], ssem.at[1], osem.at[reach], {"kv": d})
            if k:
                copy.start()
            else:
                pl.when(d != kv)(copy.start)
        ready = later
    rx2[0, xc] = tx2[kv]

    for dist in ORDER:
        if dist in (0, 1, 3):
            group = (rx2.at[0, pl.ds(0, 7)], rx2.at[pl.ds(0, 4)], None, rx2.at[pl.ds(0, 3)])[dist]
            move(group, group, ssem.at[1], osem.at[(dist + 1) // 2], {"kv": kv}).wait_recv()
        mixed_ref[:, :, pl.ds(pl.multiple_of((z + dist) % 8 * 128, 128), 128)] = jnp.transpose(
            rx2[dist].reshape(128, 128)
        ).reshape(PROPS, F, 128)
    for side, count in ((0, 8 * len(DIRECT) - 1 + 6), (1, NKV - 1)):
        sent = (tx1, tx2)[side].at[pl.ds(0, count)]
        move(sent, sent, ssem.at[side], hsem.at[0], {"kv": kv}).wait_send()
    all_passed(lambda copy: copy.wait_send())
    sent = mh_v.at[pl.ds(0, 3)]
    move(sent, sent, asem, asem, {"tp": tp}).wait_send()


def tail(mixed_v, taken_v, mixed_hbm, taken_hbm, sem):
    for i in range(8):
        part = pl.ds(2 * i, 2)
        pltpu.make_async_copy(taken_v.at[part], taken_hbm.at[part], sem.at[0]).start()
    pltpu.make_async_copy(mixed_v, mixed_hbm, sem.at[1]).start()
    pltpu.make_async_copy(taken_v, taken_hbm, sem.at[0]).wait()
    pltpu.make_async_copy(mixed_v, mixed_hbm, sem.at[1]).wait()


def shards(hidden, norm_gain, w_query, w_forget, w_input, w_outgate, w_out, floor, head_gain, base_state, prev_forget, prev_input, accepted):
    any_spec = pl.BlockSpec(memory_space=pl.ANY)
    vmem = pl.BlockSpec(memory_space=pltpu.VMEM)
    bf, f32 = jnp.bfloat16, jnp.float32
    mixed, taken = pl.pallas_call(
        kernel,
        name="verify",
        out_shape=(
            pltpu.VMEM((PROPS, F, NKV * SEQ), bf),
            pltpu.VMEM((SEQ, 2, HD, HD), f32),
        ),
        in_specs=[any_spec] * 13,
        out_specs=(vmem, vmem),
        scratch_shapes=[
            pltpu.VMEM((PROPS, F, NKV * SEQ), bf),
            pltpu.VMEM((1, D + 384), f32),
            pltpu.VMEM((4, D, 256), bf),
            pltpu.VMEM((1024, D), bf),
            pltpu.VMEM((SEQ, 2, HD, HD), f32),
            pltpu.VMEM((2, SEQ, PROPS, 256), bf),
            pltpu.VMEM((1, SEQ), jnp.int32),
            pltpu.VMEM((SEQ, 2 * HD, HD), bf),
            pltpu.VMEM((NKV, SEQ, 128), bf),
            pltpu.VMEM((8, 8, SEQ, 128), bf),
            pltpu.VMEM((4, ROWS, 256), f32),
            pltpu.VMEM((2, 8 * SEQ, HD), f32),
            pltpu.VMEM((8 * SEQ, HD), f32),
            pltpu.VMEM((NTP, 2, ROWS, HD), bf),
            pltpu.VMEM((NKV, SEQ, 128), bf),
            pltpu.VMEM((8, 8, SEQ, 128), bf),
            pltpu.VMEM((ROWS, D), f32),
            pltpu.VMEM((3, 2, SEQ, 128), bf),
            pltpu.SemaphoreType.DMA((7,)),
            pltpu.SemaphoreType.DMA((2,)),
            pltpu.SemaphoreType.DMA((3,)),
            pltpu.SemaphoreType.DMA((2,)),
            pltpu.SemaphoreType.DMA,
            pltpu.SemaphoreType.DMA,
            pltpu.SemaphoreType.DMA((3,)),
            pltpu.SemaphoreType.DMA,
            pltpu.SemaphoreType.DMA((3,)),
        ],
        compiler_params=pltpu.CompilerParams(collective_id=0, has_side_effects=True),
    )(
        jnp.transpose(hidden, (1, 2, 0)),
        norm_gain.reshape(1, -1),
        w_query, w_forget, w_input, w_outgate, w_out,
        floor.reshape(1, -1),
        head_gain.reshape(1, -1),
        base_state, prev_forget, prev_input,
        accepted.reshape(1, -1),
    )
    mixed, taken = pl.pallas_call(
        tail,
        name="place",
        out_shape=(
            jax.ShapeDtypeStruct((PROPS, F, NKV * SEQ), bf),
            jax.ShapeDtypeStruct((SEQ, 2, HD, HD), f32),
        ),
        in_specs=[vmem] * 2,
        out_specs=(any_spec,) * 2,
        scratch_shapes=[pltpu.SemaphoreType.DMA((2,))],
    )(pltpu.with_memory_space_constraint(mixed, pltpu.VMEM), pltpu.with_memory_space_constraint(taken, pltpu.VMEM))
    return jnp.transpose(mixed, (2, 0, 1)), taken


def solution(mesh):
    in_specs = (
        P(None, None, "kv"), P(), P(None, "tp"), P(None, "tp"), P(None, "tp"), P(None, "tp"), P(), P("tp"), P(),
        P("kv", "tp", None, None), P("kv", None, "tp"), P("kv", None, "tp"), P("kv"),
    )
    out_specs = (P(None, None, "kv"), P("kv", "tp", None, None))
    return jax.shard_map(shards, mesh=mesh, in_specs=in_specs, out_specs=out_specs, check_vma=False)
```

```python
import functools

import jax
import jax.numpy as jnp
from jax import lax
from jax.experimental import pallas as pl
from jax.experimental.pallas import tpu as pltpu
from jax.sharding import PartitionSpec as P

D = 2048
HD = 128
PROPS = 4
NKV = 64
NTP = 4
SEQ = 16
ROWS = SEQ * PROPS
F = D // NKV
EARLY = 8
MESH = pl.DeviceIdType.MESH
ORDER = (0, 1, 7, 2, 6, 3, 5, 4)
RELAYED = (4, 3, 5)
DIRECT = (2, 6, 1, 7, 0)
UNITS = tuple(sorted(((zt, q) for zt in range(8) for q in range(2)), key=lambda u: (min(u[0], 4) + 1.2 * u[1], u)))
HOLD = {3: 0, 5: 1, 4: 2}


def swap_blocks(parts):
    lane = lax.broadcasted_iota(jnp.int32, parts[0].shape, parts[0].ndim - 1)
    axis = parts[0].ndim - 1
    place = lane // 32
    found = []
    for i in range(4):
        block = parts[i]
        for r in range(1, 4):
            block = jnp.where(place == (i + r) % 4, pltpu.roll(parts[(i + r) % 4], 32 * r, axis), block)
        found.append(block)
    return found


def sigmoid(x):
    return jax.nn.sigmoid(x)


def kernel(
    x_hbm, gain_hbm, wq_hbm, wf_hbm, wi_hbm, wg_hbm, wo_hbm, floor_hbm, hgain_hbm,
    base_hbm, pf_hbm, pv_hbm, acc_hbm,
    mixed_ref, taken_ref,
    x_v, small_v, w_v, wo_v, base_v, pfv_v, acc_v,
    s0_v, tx1, rx1, pre_v, a_v, o_v, mh_v, tx2, rx2,
    acc_o,
    hold,
    lsem, ssem, rsem, hsem, fsem, gsem, osem, asem, bsem,
):
    kv = lax.axis_index("kv")
    tp = lax.axis_index("tp")
    z = kv // 8
    xc = kv % 8
    mine = xc % 2
    xr_base = xc // 2
    turn = [(1 * tp + 2 * mine + 2 * part + 1) % 4 for part in range(2)]
    xd = [(xr_base + 4 - turn[part]) % 4 for part in range(2)]

    barrier = pltpu.get_barrier_semaphore()
    def local(src, dst, n):
        return pltpu.make_async_copy(src, dst, lsem.at[n])

    small = ((gain_hbm, 0, D), (floor_hbm, D, 256), (hgain_hbm, D + 256, HD))
    locals_ = [
        local(x_hbm, x_v, 0),
        local(pf_hbm, pfv_v.at[0], 1),
        local(pv_hbm, pfv_v.at[1], 1),
        local(acc_hbm, acc_v, 2),
        *(local(ref, small_v.at[:, pl.ds(at, n)], 3) for ref, at, n in small),
        local(base_hbm, base_v, 4),
        *(local(ref, w_v.at[i], 5) for i, ref in enumerate((wq_hbm, wf_hbm, wi_hbm, wg_hbm))),
        local(wo_hbm, wo_v, 6),
    ]
    whole = [x_v, pfv_v, acc_v, small_v, base_v, w_v, wo_v]

    def wait_local(n):
        local(whole[n], whole[n], n).wait()

    locals_[0].start()


    def greet(where):
        pl.semaphore_signal(barrier, inc=1, device_id=where, device_id_type=MESH)

    for dist in RELAYED:
        greet({"kv": (z + dist) % 8 * 8 + xc})
    for part in range(2):
        for r in (2, 1, 3, 0):
            for m in range(2):
                core = (mine + m) % 2
                where = {"kv": z * 8 + (xr_base + r) % 4 * 2 + core, "tp": 1 * (r + 2 * core + 2 * part + 3) % 4}
                if r == 0 and m == 0:
                    pl.when(turn[part] != 0)(functools.partial(greet, where))
                else:
                    greet(where)
    for dist in DIRECT:
        for k in range(1 if dist == 0 else 0, 8):
            greet({"kv": (z + dist) % 8 * 8 + (xc + 4 + k) % 8 if dist else z * 8 + (xc + k) % 8})
    for k in range(1, NTP):
        greet({"tp": (tp + k) % NTP})

    for copy in locals_[1:]:
        copy.start()

    wait_local(0)
    for b in range(8):
        block = x_v[:, :, 128 * b : 128 * (b + 1)].reshape(128, 128)
        tx1[8 * b : 8 * (b + 1)] = jnp.transpose(block).reshape(8, SEQ, 128)

    for n in range(1, 5):
        wait_local(n)
    fl = small_v[:, D : D + 256]
    row4 = lax.broadcasted_iota(jnp.int32, (PROPS, 2 * HD), 0)
    a_v[...] = jnp.zeros_like(a_v)
    ones_row = (lax.broadcasted_iota(jnp.int32, (8, HD), 0) == 4).astype(jnp.float32)
    seq_lane = lax.broadcasted_iota(jnp.int32, (1, SEQ), 1)

    def state_step(s, c):
        count = jnp.sum(jnp.where(seq_lane == s, acc_v[...], 0), axis=1, keepdims=True)
        live = row4 < count
        f = fl + (1.0 - fl) * sigmoid(pfv_v[0, s].astype(jnp.float32))
        k = jnp.where(live, 1.0 - f, 0.0)
        f = jnp.where(live, f, 1.0)
        v = pfv_v[1, s].astype(jnp.float32)
        f0, f1, f2, f3 = (f[j : j + 1] for j in range(4))
        f23 = f2 * f3
        f123 = f1 * f23
        coef = jnp.concatenate(
            [k[0:1] * f123, k[1:2] * f23, k[2:3] * f3, k[3:4], f0 * f123, jnp.zeros((3, 2 * HD), jnp.float32)],
            axis=0,
        )
        high = coef.astype(jnp.bfloat16).astype(jnp.float32)
        rest = coef - high
        mid = rest.astype(jnp.bfloat16).astype(jnp.float32)
        lhs = jnp.concatenate([high, mid, rest - mid, jnp.zeros((8, 2 * HD), jnp.float32)], axis=0).astype(jnp.bfloat16)
        for h in range(2):
            cols = slice(h * HD, (h + 1) * HD)
            rows = jnp.concatenate([v[:, cols], jnp.zeros((4, HD), jnp.float32)], axis=0)
            rows = jnp.concatenate([ones_row, rows], axis=1)
            rhs = jnp.concatenate([rows] * 4, axis=0).astype(jnp.bfloat16)
            spread = lax.dot_general(
                lhs[:, cols], rhs, (((0,), (0,)), ((), ())), preferred_element_type=jnp.float32
            )
            new = spread[:, :HD] * base_v[s, h] + spread[:, HD:]
            taken_ref[s, h] = new
            s0_v[s, cols, :] = new.astype(jnp.bfloat16)
        return c

    lax.fori_loop(0, EARLY, state_step, 0, unroll=4)

    others = (turn[0] + 3) // 4 + (turn[1] + 3) // 4
    pl.semaphore_wait(barrier, 8 * len(DIRECT) - 1 + len(RELAYED) + NTP - 1 + 14 + others)


    def move(src, dst, send_sem, recv_sem, where):
        return pltpu.make_async_remote_copy(
            src_ref=src, dst_ref=dst, send_sem=send_sem, recv_sem=recv_sem, device_id=where, device_id_type=MESH
        )

    def send_relayed(dist):
        zd = (z + dist) % 8
        slot = HOLD[8 - dist]
        move(
            tx1.at[pl.ds(zd * 8 + xd[slot // 2] * 2, 2)], hold.at[slot], ssem.at[0], hsem.at[slot // 2],
            {"kv": zd * 8 + xc},
        ).start()

    def send_direct(side, dist):
        tx, rx = ((tx1, rx1), (tx2, rx2))[side]
        zd = (z + dist) % 8
        slot = ORDER.index((8 - dist) % 8)
        for k in range(1 if dist == 0 else 0, 8):
            d = zd * 8 + (xc + k) % 8
            move(tx.at[d], rx.at[slot, xc], ssem.at[side], rsem.at[(slot + 1) // 2], {"kv": d}).start()

    def other(k):
        return tp if k == 3 else k + (k - tp + 4) // 4

    def pass_on(part):
        held = hold.at[pl.ds(2 * part, 2 - part)]
        to = rx1.at[pl.ds(5 + 2 * part, 2 - part)]
        move(held, held, ssem.at[0], hsem.at[part], {"kv": kv}).wait_recv()
        for m in range(2):
            core = (mine + m) % 2
            for k in range(NTP):
                copy = move(
                    held.at[:, core], to.at[:, xc], fsem, gsem,
                    {"kv": z * 8 + xd[part] * 2 + core, "tp": other(k)},
                )
                if m == 0 and k == 3:
                    pl.when(turn[part] != 0)(copy.start)

                    @pl.when(turn[part] == 0)
                    def _():
                        for b in range(2 - part):
                            rx1[5 + 2 * part + b, xc] = hold[2 * part + b, core]
                else:
                    copy.start()

    def all_passed(wait):
        for when, blocks in ((turn[0] == 0, 22), (turn[1] == 0, 23), (turn[0] * turn[1] != 0, 24)):
            some = tx1.at[pl.ds(0, blocks)]
            pl.when(when)(functools.partial(wait, move(some, some, fsem, gsem, {"kv": kv})))

    def wait_direct(part):
        group = rx1.at[pl.ds(1, 2)] if part else rx1.at[0, pl.ds(0, 7)]
        move(group, group, ssem.at[0], rsem.at[part], {"kv": kv}).wait_recv()

    for dist in RELAYED:
        send_relayed(dist)
    rx1[0, xc] = tx1[kv]

    lax.fori_loop(EARLY, SEQ, state_step, 0, unroll=4)
    for dist in DIRECT:
        send_direct(0, dist)
    pass_on(0)
    pass_on(1)
    wait_local(5)
    squares = jnp.zeros((SEQ, 128), jnp.float32)

    def take(n):
        zs = (z + ORDER[n]) % 8
        vals = rx1[n].astype(jnp.float32)
        tiles = []
        for q in range(2):
            swapped = swap_blocks([vals[4 * q + i] for i in range(4)])
            gain = small_v[:, pl.ds(pl.multiple_of(zs * 256 + q * 128, 128), 128)]
            tiles.append(jnp.concatenate([(part * gain).astype(jnp.bfloat16) for part in swapped], axis=0))
        lhs = jnp.concatenate(tiles, axis=1)
        prods = [
            jnp.dot(lhs, w_v[i, pl.ds(pl.multiple_of(zs * 256, 256), 256), :], preferred_element_type=jnp.float32)
            for i in range(4)
        ]
        return jnp.sum(vals * vals, axis=0), prods

    for n in range(5):
        if n in (0, 1, 3):
            wait_direct((n + 1) // 2)
        part, prods = take(n)
        squares = squares + part
        for i in range(4):
            if n == 0:
                pre_v[i] = prods[i]
            else:
                pre_v[i] += prods[i]
    all_passed(lambda copy: copy.wait_recv())
    last = [take(n) for n in (5, 6, 7)]
    squares = squares + last[0][0] + last[1][0] + last[2][0]
    sums = [pre_v[i] + (last[0][1][i] + last[1][1][i] + last[2][1][i]) for i in range(4)]
    lane = lax.broadcasted_iota(jnp.int32, (SEQ, 128), 1)
    scale = jnp.concatenate(
        [
            lax.rsqrt(
                jnp.sum(jnp.where(lane // F == p, squares, 0.0), axis=1, keepdims=True) / D + 1e-06
            )
            for p in range(PROPS)
        ],
        axis=0,
    )

    def pre(i):
        return (sums[i] * scale).astype(jnp.bfloat16).astype(jnp.float32)

    q_all = pre(0)
    q_all = q_all * sigmoid(q_all)
    f_all = fl + (1.0 - fl) * sigmoid(pre(1))
    k_all = 1.0 - f_all
    v_all = pre(2)

    def at(arr, t):
        return arr[t * SEQ : (t + 1) * SEQ]

    decay = None
    for t in range(PROPS):
        decay = at(f_all, t) if t == 0 else decay * at(f_all, t)
        scaled = at(q_all, t) * decay
        for h in range(2):
            a_v[h, pl.ds(4 * h + t, SEQ, stride=8), :] = scaled[:, h * HD : (h + 1) * HD]
    for s in range(SEQ):
        lhs = jnp.concatenate([a_v[0, 8 * s : 8 * s + 8], a_v[1, 8 * s : 8 * s + 8]], axis=1).astype(jnp.bfloat16)
        o_v[8 * s : 8 * s + 8] = jnp.dot(lhs, s0_v[s], preferred_element_type=jnp.float32)
    hg = small_v[:, D + 256 : D + 384]
    gate = pre(3)
    gate = gate * sigmoid(gate)
    for h in range(2):
        cols = slice(h * HD, (h + 1) * HD)
        for t in range(PROPS):
            weight = at(q_all, t)[:, cols]
            o = o_v[pl.ds(4 * h + t, SEQ, stride=8), :]
            for j in range(t, -1, -1):
                o = o + jnp.sum(weight * at(k_all, j)[:, cols], axis=1, keepdims=True) * at(v_all, j)[:, cols]
                if j:
                    weight = weight * at(f_all, j)[:, cols]
            norm = lax.rsqrt(jnp.mean(o * o, axis=1, keepdims=True) + 1e-05)
            mh_v[tp, h, t * SEQ : (t + 1) * SEQ, :] = (o * norm * hg * at(gate, t)[:, cols]).astype(jnp.bfloat16)
        for k in range(3):
            there = mh_v.at[tp, h]
            move(there, there, asem, bsem.at[(other(k) - tp + 3) % NTP], {"tp": other(k)}).start()

    def wait_gather(k):
        there = mh_v.at[(tp - k + NTP) % NTP]
        move(there, there, asem, bsem.at[k - 1], {"tp": tp}).wait_recv()

    wait_local(6)

    def piece(k, cols):
        place = (tp - k + NTP) % NTP
        w = wo_v[pl.ds(pl.multiple_of(place * 256, 256), 256), cols]
        return jnp.dot(jnp.concatenate([mh_v[place, 0], mh_v[place, 1]], axis=1), w, preferred_element_type=jnp.float32)

    for k in (0, 1, 3):
        if k:
            wait_gather(k)
        for n in range(4):
            cols = slice(n * 512, (n + 1) * 512)
            if k:
                acc_o[:, cols] += piece(k, cols)
            else:
                acc_o[:, cols] = piece(k, cols)
    wait_gather(2)

    def product(first, tiles):
        cols = pl.ds(pl.multiple_of(first * F, 128), tiles * 128)
        return acc_o[:, cols] + piece(2, cols)

    def blocks_of(out):
        found = []
        for q in range(out.shape[1] // 128):
            parts = [out[p * SEQ : (p + 1) * SEQ, q * 128 : (q + 1) * 128] for p in range(PROPS)]
            found += [part.astype(jnp.bfloat16) for part in swap_blocks(parts)]
        return found

    chunks = [(zt * 8 + 4 * q, 1) for zt, q in UNITS]
    outs = [product(*chunks[0]), product(*chunks[1])]
    ready = blocks_of(outs[0])
    for n, (first, _) in enumerate(chunks):
        if n + 2 < len(chunks):
            outs.append(product(*chunks[n + 2]))
        later = blocks_of(outs[n + 1]) if n + 1 < len(chunks) else None
        for j, block in enumerate(ready):
            tx2[first + j] = block
        zt, q = UNITS[n]
        slot = (z + 8 - zt) % 8
        reach = (slot * (8 - slot) + 1) // 8
        for k in range(4):
            d = first + (xc + k) % 4
            copy = move(tx2.at[d], rx2.at[slot, xc], ssem.at[1], osem.at[reach], {"kv": d})
            if k:
                copy.start()
            else:
                pl.when(d != kv)(copy.start)
        ready = later
    rx2[0, xc] = tx2[kv]

    for dist in ORDER:
        if dist in (0, 1, 3):
            group = (rx2.at[0, pl.ds(0, 7)], rx2.at[pl.ds(0, 4)], None, rx2.at[pl.ds(0, 3)])[dist]
            move(group, group, ssem.at[1], osem.at[(dist + 1) // 2], {"kv": kv}).wait_recv()
        mixed_ref[:, :, pl.ds(pl.multiple_of((z + dist) % 8 * 128, 128), 128)] = jnp.transpose(
            rx2[dist].reshape(128, 128)
        ).reshape(PROPS, F, 128)
    for side, count in ((0, 8 * len(DIRECT) - 1 + 6), (1, NKV - 1)):
        sent = (tx1, tx2)[side].at[pl.ds(0, count)]
        move(sent, sent, ssem.at[side], hsem.at[0], {"kv": kv}).wait_send()
    all_passed(lambda copy: copy.wait_send())
    sent = mh_v.at[pl.ds(0, 3)]
    move(sent, sent, asem, asem, {"tp": tp}).wait_send()


def tail(mixed_v, taken_v, mixed_hbm, taken_hbm, sem):
    for i in range(8):
        part = pl.ds(2 * i, 2)
        pltpu.make_async_copy(taken_v.at[part], taken_hbm.at[part], sem.at[0]).start()
    pltpu.make_async_copy(mixed_v, mixed_hbm, sem.at[1]).start()
    pltpu.make_async_copy(taken_v, taken_hbm, sem.at[0]).wait()
    pltpu.make_async_copy(mixed_v, mixed_hbm, sem.at[1]).wait()


def shards(hidden, norm_gain, w_query, w_forget, w_input, w_outgate, w_out, floor, head_gain, base_state, prev_forget, prev_input, accepted):
    any_spec = pl.BlockSpec(memory_space=pl.ANY)
    vmem = pl.BlockSpec(memory_space=pltpu.VMEM)
    bf, f32 = jnp.bfloat16, jnp.float32
    mixed, taken = pl.pallas_call(
        kernel,
        name="verify",
        out_shape=(
            pltpu.VMEM((PROPS, F, NKV * SEQ), bf),
            pltpu.VMEM((SEQ, 2, HD, HD), f32),
        ),
        in_specs=[any_spec] * 13,
        out_specs=(vmem, vmem),
        scratch_shapes=[
            pltpu.VMEM((PROPS, F, NKV * SEQ), bf),
            pltpu.VMEM((1, D + 384), f32),
            pltpu.VMEM((4, D, 256), bf),
            pltpu.VMEM((1024, D), bf),
            pltpu.VMEM((SEQ, 2, HD, HD), f32),
            pltpu.VMEM((2, SEQ, PROPS, 256), bf),
            pltpu.VMEM((1, SEQ), jnp.int32),
            pltpu.VMEM((SEQ, 2 * HD, HD), bf),
            pltpu.VMEM((NKV, SEQ, 128), bf),
            pltpu.VMEM((8, 8, SEQ, 128), bf),
            pltpu.VMEM((4, ROWS, 256), f32),
            pltpu.VMEM((2, 8 * SEQ, HD), f32),
            pltpu.VMEM((8 * SEQ, HD), f32),
            pltpu.VMEM((NTP, 2, ROWS, HD), bf),
            pltpu.VMEM((NKV, SEQ, 128), bf),
            pltpu.VMEM((8, 8, SEQ, 128), bf),
            pltpu.VMEM((ROWS, D), f32),
            pltpu.VMEM((3, 2, SEQ, 128), bf),
            pltpu.SemaphoreType.DMA((7,)),
            pltpu.SemaphoreType.DMA((2,)),
            pltpu.SemaphoreType.DMA((3,)),
            pltpu.SemaphoreType.DMA((2,)),
            pltpu.SemaphoreType.DMA,
            pltpu.SemaphoreType.DMA,
            pltpu.SemaphoreType.DMA((3,)),
            pltpu.SemaphoreType.DMA,
            pltpu.SemaphoreType.DMA((3,)),
        ],
        compiler_params=pltpu.CompilerParams(collective_id=0, has_side_effects=True),
    )(
        jnp.transpose(hidden, (1, 2, 0)),
        norm_gain.reshape(1, -1),
        w_query, w_forget, w_input, w_outgate, w_out,
        floor.reshape(1, -1),
        head_gain.reshape(1, -1),
        base_state, prev_forget, prev_input,
        accepted.reshape(1, -1),
    )
    mixed, taken = pl.pallas_call(
        tail,
        name="place",
        out_shape=(
            jax.ShapeDtypeStruct((PROPS, F, NKV * SEQ), bf),
            jax.ShapeDtypeStruct((SEQ, 2, HD, HD), f32),
        ),
        in_specs=[vmem] * 2,
        out_specs=(any_spec,) * 2,
        scratch_shapes=[pltpu.SemaphoreType.DMA((2,))],
    )(pltpu.with_memory_space_constraint(mixed, pltpu.VMEM), pltpu.with_memory_space_constraint(taken, pltpu.VMEM))
    return jnp.transpose(mixed, (2, 0, 1)), taken


def solution(mesh):
    in_specs = (
        P(None, None, "kv"), P(), P(None, "tp"), P(None, "tp"), P(None, "tp"), P(None, "tp"), P(), P("tp"), P(),
        P("kv", "tp", None, None), P("kv", None, "tp"), P("kv", None, "tp"), P("kv"),
    )
    out_specs = (P(None, None, "kv"), P("kv", "tp", None, None))
    return jax.shard_map(shards, mesh=mesh, in_specs=in_specs, out_specs=out_specs, check_vma=False)
```
